32 devices in a mesh: fs: 8 (over z, y), tp: 4 (over x, core).
Axes of the slice: x: 2, y: 2, z: 4, core: 2. Of those that a mesh axis runs over, the one named last changes fastest.
Arguments:
- tokens: bfloat16 [4096, 2048], P(('fs', 'tp')), may hold values from -6 to 6
- routes: int32 [4096, 4], P(('fs', 'tp')), may hold values from 0 to 31, all different within a row; in each aligned block of 128 rows (0 to 127, 128 to 255, ...) at most 24 rows name the same one
- route_weight: float32 [4096, 4], P(('fs', 'tp')), may hold values from 0.1 to 1
- norm_gain: float32 [2048], P('fs'), may hold values from 0.5 to 4
- gate_weight: float32 [32, 2048, 512], P(None, 'fs', 'tp'), may hold values from -0.125 to 0.125
- up_weight: float32 [32, 2048, 512], P(None, 'fs', 'tp'), may hold values from -0.125 to 0.125
- down_weight: float32 [32, 512, 2048], P(None, 'fs', 'tp'), may hold values from -0.0625 to 0.0625
Outputs:
- gate_new: bfloat16 [32, 2048, 512], P(('fs', 'tp'))
- up_new: bfloat16 [32, 2048, 512], P(('fs', 'tp'))
- down_new: bfloat16 [32, 512, 2048], P(('fs', 'tp'))
- mixed: bfloat16 [4096, 2048], P(('fs', 'tp'))
The draws below stay inside these ranges and needn't reach their ends.
Inputs may be any that keep to these rules, and one draw needn't show every extreme that they name: `routes`: each row names 4 different experts, and every expert is named by some row; within the 128 rows of one device no expert is named by more than 24 rows, and in some blocks an expert is named by exactly 24 rows.
All inputs are finite; a program needn't handle non-finite values.
Results may differ from the reference program's by a relative error of at most 0.0084.
Values may be sent and summed in bfloat16 or wider, within the bound.
A program may use at most 128 MiB of HBM per device.

```python
import math
import jax
import jax.numpy as jnp
import numpy as np
from jax import lax

D = 2048
FF = 512
TOP_K = 4
TOK_DEV = 128
EXPERTS = 32
CAP = 24
TOKENS = 4096
N_FS = 8
N_TP = 4


def shard_levels(rng, shape, shards, least, largest):
    loudness, own = 1.0, jax.random.fold_in(rng, 6)
    for position, parts in shards:
        draws = jnp.exp(jax.random.uniform(jax.random.fold_in(own, position), (parts,), jnp.float32, least / len(shards), largest / len(shards)))
        loudness = loudness * jnp.repeat(draws, shape[position] // parts).reshape([-1 if axis == position else 1 for axis in range(len(shape))])
    return loudness


def shared_out(rng, own, number, rows, amount, top, reach, skew):
    ranking = jax.random.permutation(rng, amount)
    heavy_load, usual = portions_of(amount, rows * top, reach, skew, True), portions_of(amount, rows * top, reach, skew, False)
    places = jnp.arange(amount)

    def named(lengths, turn):
        used = int((lengths > 0).sum())
        fixed = max(1, used // 4)
        shifted = fixed + (places - fixed + turn * (used - fixed)) % max(1, amount - fixed)
        return jnp.zeros((amount,), jnp.int32).at[ranking[jnp.where(places < fixed, places, shifted)]].set(jnp.asarray(lengths, jnp.int32))

    lengths = jnp.where(number % 4 == 0, named(heavy_load, number // 4), named(usual, number - number // 4 - 1))
    mixed = jax.random.permutation(jax.random.fold_in(own, 3), amount)
    giver, sink = mixed[0:amount // 2 * 2:2], mixed[1:amount // 2 * 2:2]
    slack = jnp.minimum(lengths[giver] - 1, reach - lengths[sink]) // 2
    slack = jnp.where((giver == ranking[0]) | (sink == ranking[0]) | (lengths[sink] == 0), 0, jnp.maximum(slack, 0))
    shifted = jax.random.randint(jax.random.fold_in(own, 4), (amount // 2,), 0, 1 << 20) % (slack + 1)
    lengths = lengths.at[giver].add(-shifted).at[sink].add(shifted)
    members = jnp.searchsorted(jnp.cumsum(lengths), jnp.arange(rows * top), side="right").astype(jnp.int32)
    listing = members.reshape(top, rows).T
    listing = listing[jax.random.permutation(jax.random.fold_in(own, 1), rows)]
    turn = jax.random.randint(jax.random.fold_in(own, 2), (rows, 1), 0, top)
    return jnp.take_along_axis(listing, (jnp.arange(top)[None, :] + turn) % top, axis=1)


def portions_of(number_of, total, most, lean, full):
    weights = [(1 << 20) // math.isqrt(rank ** lean) + 1 for rank in range(1, number_of + 1)]
    largest = most if full else min(most, max(-(-total // number_of), total * weights[0] // sum(weights)))
    least = 1 if total - largest >= number_of - 1 else 0
    given, rest = [largest] + [least] * (number_of - 1), total - largest - least * (number_of - 1)
    while rest > 0:
        free = [i for i in range(1, number_of) if given[i] < largest] or [i for i in range(1, number_of) if given[i] < most]
        whole, remaining = sum([weights[i] for i in free]), rest
        for i in free:
            extra = min(most - given[i], max(1, remaining * weights[i] // whole), rest)
            given[i] = given[i] + extra
            rest = rest - extra
    return np.array(given)


def noise(stream_key, shape, deviation, most, split=(), held_as=jnp.bfloat16):
    values = jax.random.normal(stream_key, shape, jnp.float32) * deviation
    if len(split) > 0:
        values = shard_levels(stream_key, shape, split, -0.22, 0.18) * values
    return jnp.clip(values, min=-most, max=most).astype(held_as)


def setup_inputs(seed: int = 0) -> dict:
    streams_of = jax.random.split(jax.random.key(seed), 8)
    tokens = noise(streams_of[0], (TOKENS, D), 1.0, 6.0, ((0, 32),))
    routes_keys = jax.random.split(jax.random.fold_in(streams_of[1], 1), TOKENS // TOK_DEV)
    routes_turns = jax.random.permutation(jax.random.fold_in(streams_of[1], 3), TOKENS // TOK_DEV)
    routes = jax.vmap(lambda own, number: shared_out(jax.random.fold_in(streams_of[1], 2), own, number, TOK_DEV, EXPERTS, TOP_K, CAP, 1))(routes_keys, routes_turns).reshape((TOKENS, TOP_K))
    route_weight = jnp.clip(jnp.exp(math.log(1.0) - 2.3025851 * jax.random.uniform(streams_of[2], (TOKENS, TOP_K), jnp.float32) ** shard_levels(streams_of[2], (TOKENS, TOP_K), ((0, 32),), -0.2, 0.2)), 0.1, 1.0)
    norm_gain = jnp.clip(jnp.exp(math.log(4.0) - 2.0794415 * jax.random.uniform(streams_of[3], (D,), jnp.float32) ** shard_levels(streams_of[3], (D,), ((0, 8),), -0.2, 0.2)), 0.5, 4.0)
    gate_weight = noise(streams_of[4], (EXPERTS, D, FF), D ** -0.5, 0.125, ((1, 8), (2, 4)), jnp.float32)
    up_weight = noise(streams_of[5], (EXPERTS, D, FF), D ** -0.5, 0.125, ((1, 8), (2, 4)), jnp.float32)
    down_weight = noise(streams_of[6], (EXPERTS, FF, D), (16 * FF) ** -0.5, 0.0625, ((1, 8), (2, 4)), jnp.float32)
    return {"tokens": tokens, "routes": routes, "route_weight": route_weight, "norm_gain": norm_gain, "gate_weight": gate_weight, "up_weight": up_weight, "down_weight": down_weight}


norm_epsilon = 1e-06
clamp_limit = 7.0
sigmoid_slope = 1.702

def feed(inputs, gate_mat, up_mat, down_mat):
    gate_pre = jnp.dot(inputs, gate_mat, preferred_element_type=jnp.float32)
    up_pre = jnp.dot(inputs, up_mat, preferred_element_type=jnp.float32)
    gate_part = jnp.minimum(gate_pre, clamp_limit)
    linear_part = jnp.clip(up_pre, -clamp_limit, clamp_limit)
    activation = (gate_part * jax.nn.sigmoid(sigmoid_slope * gate_part) * (linear_part + 1.0)).astype(jnp.bfloat16)
    return jnp.dot(activation, down_mat, preferred_element_type=jnp.float32).astype(jnp.bfloat16)

def reference(tokens, routes, route_weight, norm_gain, gate_weight, up_weight, down_weight):
    gate_all = (gate_weight * norm_gain[None, :, None]).astype(jnp.bfloat16)
    up_all = (up_weight * norm_gain[None, :, None]).astype(jnp.bfloat16)
    down_all = down_weight.astype(jnp.bfloat16)
    values = tokens.astype(jnp.float32)
    squares = lax.optimization_barrier(jnp.mean(values * values, axis=1, keepdims=True))
    normed = (values * lax.rsqrt(squares + norm_epsilon)).astype(jnp.bfloat16)
    devices = N_FS * N_TP
    pair_experts = routes.reshape(devices, TOK_DEV * TOP_K)
    onehot = (pair_experts[:, :, None] == jnp.arange(EXPERTS, dtype=jnp.int32)[None, None, :]).astype(jnp.int32)
    earlier = jnp.cumsum(onehot, axis=1) - onehot
    rank = lax.optimization_barrier(jnp.sum(earlier * onehot, axis=2)).astype(jnp.int32)
    source_dev = jnp.arange(devices, dtype=jnp.int32)[:, None]
    column = (source_dev * CAP + rank).astype(jnp.int32)
    token_index = (source_dev * TOK_DEV + jnp.arange(TOK_DEV * TOP_K, dtype=jnp.int32)[None, :] // TOP_K).astype(jnp.int32)
    slot_table = jnp.full((EXPERTS, devices * CAP), TOKENS, jnp.int32).at[pair_experts, column].set(token_index)
    padded = jnp.concatenate([normed, jnp.zeros((1, D), jnp.bfloat16)], axis=0)

    def expert_rows(operands):
        rows_index, gate_mat, up_mat, down_mat = operands
        return feed(padded[rows_index], gate_mat, up_mat, down_mat)
    returned = lax.map(expert_rows, (slot_table, gate_all, up_all, down_all))
    picked = returned[pair_experts, column].reshape(TOKENS, TOP_K, D)
    mixed = lax.optimization_barrier(jnp.sum(picked.astype(jnp.float32) * route_weight[:, :, None], axis=1)).astype(jnp.bfloat16)
    return (gate_all, up_all, down_all, mixed)
```

```python
import functools

import jax
import jax.numpy as jnp
from jax import lax
from jax.experimental import pallas as pl
from jax.experimental.pallas import tpu as pltpu
from jax.sharding import PartitionSpec as P

norm_epsilon = 1e-06
clamp_limit = 7.0
sigmoid_slope = 1.702
MESH = pl.DeviceIdType.MESH


def feed(inputs, gate_mat, up_mat, down_mat):
    gate_pre = jnp.dot(inputs, gate_mat, preferred_element_type=jnp.float32)
    up_pre = jnp.dot(inputs, up_mat, preferred_element_type=jnp.float32)
    gate_part = jnp.minimum(gate_pre, clamp_limit)
    linear_part = jnp.clip(up_pre, -clamp_limit, clamp_limit)
    activation = (
        gate_part * jax.nn.sigmoid(sigmoid_slope * gate_part) * (linear_part + 1.0)
    ).astype(jnp.bfloat16)
    return jnp.dot(activation, down_mat, preferred_element_type=jnp.float32).astype(jnp.bfloat16)


def assemble(received, rows_groups, column_groups):
    tile_rows = received.shape[2]
    tile_columns = received.shape[3]
    sources = received.reshape(rows_groups, column_groups, tile_rows, tile_columns)
    return sources.transpose(0, 2, 1, 3).reshape(
        1, rows_groups * tile_rows, column_groups * tile_columns
    )


def shards(tokens, routes, route_weight, norm_gain, gate_weight, up_weight, down_weight):
    gain_column = norm_gain[None, :, None]
    gate_tiles = (gate_weight * gain_column).astype(jnp.bfloat16)
    up_tiles = (up_weight * gain_column).astype(jnp.bfloat16)
    down_tiles = down_weight.astype(jnp.bfloat16)
    rows_groups = lax.axis_size("fs")
    column_groups = lax.axis_size("tp")
    arrived = (
        lax.all_to_all(gate_tiles[:, None], ("fs", "tp"), split_axis=0, concat_axis=1, tiled=True),
        lax.all_to_all(up_tiles[:, None], ("fs", "tp"), split_axis=0, concat_axis=1, tiled=True),
        lax.all_to_all(down_tiles[:, None], ("fs", "tp"), split_axis=0, concat_axis=1, tiled=True),
    )
    gate_new = assemble(arrived[0], rows_groups, column_groups)
    up_new = assemble(arrived[1], rows_groups, column_groups)
    down_new = assemble(arrived[2], rows_groups, column_groups)
    experts = rows_groups * column_groups
    tok_rows, model_width = tokens.shape
    per_token = routes.shape[1]
    capacity = max(2, 3 * tok_rows * per_token // (2 * experts))
    values = tokens.astype(jnp.float32)
    squares = jnp.mean(values * values, axis=1, keepdims=True)
    normed = (values * lax.rsqrt(squares + norm_epsilon)).astype(jnp.bfloat16)
    flat_routes = routes.reshape(-1)
    onehot = (flat_routes[:, None] == jnp.arange(experts, dtype=jnp.int32)[None, :]).astype(
        jnp.int32
    )
    earlier = jnp.cumsum(onehot, axis=0) - onehot
    rank = jnp.sum(earlier * onehot, axis=1)
    slot_index = flat_routes * capacity + rank
    slot_numbers = jnp.arange(experts * capacity, dtype=jnp.int32)
    select = jnp.any(
        slot_index.reshape(tok_rows, per_token)[None, :, :] == slot_numbers[:, None, None], axis=2
    )
    buffer = jnp.dot(
        select.astype(jnp.bfloat16), normed, preferred_element_type=jnp.float32
    ).astype(jnp.bfloat16)
    buffer = buffer.reshape(experts, 1, capacity, model_width)
    slot_rows = lax.all_to_all(buffer, ("fs", "tp"), split_axis=0, concat_axis=1, tiled=True)
    sources = slot_rows.shape[1]
    count = slot_rows.shape[2]
    expert_out = feed(slot_rows.reshape(-1, model_width), gate_new[0], up_new[0], down_new[0])
    expert_out = expert_out.reshape(1, sources, count, model_width)
    returned = lax.all_to_all(expert_out, ("fs", "tp"), split_axis=1, concat_axis=0, tiled=True)
    returned = returned.reshape(experts * capacity, model_width)
    picked = returned[slot_index].reshape(tok_rows, per_token, model_width)
    mixed = jnp.sum(picked.astype(jnp.float32) * route_weight[:, :, None], axis=1).astype(
        jnp.bfloat16
    )
    return (gate_new, up_new, down_new, mixed)


def exchange_kernel(
    sizes, tokens, routes_t, weight_t, gain, gate, up, down,
    gate_out, up_out, down_out, mixed,
    gate_in, up_in, down_in, gains, in_tiles, out_tiles, in_mats, out_mat,
    arrived, normed, slots_out, slots_in, active, far_routes, far_weight,
    mix_high, mix_low, rows_out, rows_in, part_out, part_in,
    load_sem, store_sem, token_send, token_recv, route_send, route_recv,
    first_send, first_recv, near_send, near_recv, slot_send, slot_recv,
    second_send, second_recv, back_send, back_recv, part_send, part_recv,
):
    n_fs, n_tp, capacity = sizes
    n = n_fs * n_tp
    fs, tp = lax.axis_index("fs"), lax.axis_index("tp")
    tok_rows, width = tokens.shape
    tile_rows, tile_cols = gate_in.shape[1:]
    chunks, down_rows, lanes = out_tiles.shape[1:]
    down_cols = chunks * lanes
    block = n_tp * lanes
    per_token = routes_t.shape[0]

    planes = 4
    plane_fs = n_fs // planes
    plane = n // planes
    layer, place = fs // plane_fs, lax.rem(fs, plane_fs)
    spot = place * n_tp + tp

    def flip(turn):
        low = lax.rem(layer + turn, 2)
        high = lax.rem(layer // 2 + turn // 2, 2)
        return 2 * high + low

    def device(turn, shift):
        to_place = lax.rem(place + shift // n_tp, plane_fs)
        to_tp = lax.rem(tp + lax.rem(shift, n_tp), n_tp)
        return flip(turn) * plane_fs + to_place, to_tp, to_place * n_tp + to_tp

    def peer(step):
        turn = lax.rem(step // (n // 2) + 1, 2) * 2 + lax.rem(step, 2)
        to_fs, to_tp, _ = device(turn, lax.rem(step // 2, plane))
        return to_fs, to_tp, to_fs * n_tp + to_tp

    def remote(source, target, send, recv, to):
        return pltpu.make_async_remote_copy(
            src_ref=source,
            dst_ref=target,
            send_sem=send,
            recv_sem=recv,
            device_id=(to[0], to[1]),
            device_id_type=MESH,
        )

    barrier = pltpu.get_barrier_semaphore()

    def greet(step, carry):
        to = peer(lax.rem(step + n // 2 + 1, n))
        pl.semaphore_signal(barrier, inc=1, device_id=(to[0], to[1]), device_id_type=MESH)
        return carry

    loads = [
        pltpu.make_async_copy(gate, gate_in, load_sem.at[0]),
        pltpu.make_async_copy(up, up_in, load_sem.at[1]),
        pltpu.make_async_copy(down, down_in, load_sem.at[2]),
    ]
    for load in loads:
        load.start()
    lax.fori_loop(0, n - 1, greet, 0)

    for i in range(tile_rows // lanes):
        gains[i * lanes : (i + 1) * lanes, :] = jnp.transpose(
            jnp.broadcast_to(gain[i : i + 1, :], (tile_cols, lanes))
        )

    def token_copy(turn, source):
        to = 1 if turn == 3 else turn
        return remote(
            source, arrived.at[turn - 1], token_send.at[turn - 1], token_recv.at[turn - 1], device(to, 0)
        )

    def route_copy(turn):
        return remote(
            routes_t, far_routes.at[turn - 1], route_send.at[turn - 1], route_recv.at[turn - 1], device(turn, 0)
        )

    weight_copy = remote(weight_t, far_weight, route_send.at[3], route_recv.at[3], device(2, 0))
    token_copies = [
        token_copy(1, tokens),
        token_copy(2, tokens),
        token_copy(3, arrived.at[1]),
    ]
    route_copies = [route_copy(1), route_copy(2), route_copy(3), weight_copy]

    def first_copy(to):
        return remote(
            in_tiles.at[to[2]],
            in_mats.at[
                :,
                pl.ds(pl.multiple_of(fs * tile_rows, tile_rows), tile_rows),
                pl.ds(pl.multiple_of(tp * tile_cols, tile_cols), tile_cols),
            ],
            first_send,
            first_recv,
            to,
        )

    own_rows = pl.ds(pl.multiple_of(fs * down_rows, down_rows), down_rows)
    own_lanes = pl.ds(pl.multiple_of(tp * lanes, lanes), lanes)

    def near_copy(to):
        return remote(
            out_tiles.at[to[2]], out_mat.at[:, own_rows, own_lanes], near_send, near_recv, to
        )

    def second_copy(c, to):
        return remote(
            out_tiles.at[to[2], c],
            out_mat.at[c, own_rows, own_lanes],
            second_send.at[c],
            second_recv.at[c],
            to,
        )

    def cast_first(step):
        e = peer(step)[2]
        in_tiles[e, 0] = (gate_in[e] * gains[...]).astype(jnp.bfloat16)
        in_tiles[e, 1] = (up_in[e] * gains[...]).astype(jnp.bfloat16)

    def cast_second(step):
        e = peer(step)[2]
        for c in range(chunks):
            out_tiles[e, c] = down_in[e, :, c * lanes : (c + 1) * lanes].astype(jnp.bfloat16)

    def send_first(step, carry):
        cast_first(step + 1)
        first_copy(peer(step)).start()
        return carry

    before = (
        lax.broadcasted_iota(jnp.int32, (tok_rows, tok_rows), 0)
        < lax.broadcasted_iota(jnp.int32, (tok_rows, tok_rows), 1)
    ).astype(jnp.float32).astype(jnp.bfloat16)

    def named_in(turn, paths, shares):
        experts = lax.broadcasted_iota(jnp.int32, (plane, tok_rows), 0) + flip(turn) * plane
        named = jnp.zeros((plane, tok_rows), jnp.float32)
        scaled = jnp.zeros((plane, tok_rows), jnp.float32)
        for k in range(per_token):
            hit = paths[k : k + 1, :] == experts
            named = named + hit.astype(jnp.float32)
            if shares is not None:
                scaled = scaled + jnp.where(hit, shares[k : k + 1, :], 0.0)
        rank = jnp.dot(named.astype(jnp.bfloat16), before, preferred_element_type=jnp.float32)
        rank = jnp.where(named > 0.5, rank, -1.0)
        number = lax.broadcasted_iota(jnp.int32, (plane, capacity, tok_rows), 1).astype(jnp.float32)
        return (rank[:, None, :] == number).astype(jnp.float32), scaled

    def normalize(turn, rows_ref):
        values = rows_ref[...].astype(jnp.float32)
        squares = jnp.mean(values * values, axis=1, keepdims=True)
        normed[turn] = (values * lax.rsqrt(squares + norm_epsilon)).astype(jnp.bfloat16)

    def fill_slots(turn, paths):
        select, _ = named_in(0, paths, None)
        rows = jnp.dot(
            select.reshape(plane * capacity, tok_rows).astype(jnp.bfloat16),
            normed[turn],
            preferred_element_type=jnp.float32,
        )
        slots_out[:, turn] = rows.reshape(plane, capacity, width).astype(jnp.bfloat16)

    def fill_mix(q, paths, shares):
        for turn in range(2):
            select, scaled = named_in(turn, paths, shares)
            picks = jnp.transpose(
                (select * scaled[:, None, :]).reshape(plane * capacity, tok_rows)
            )
            high = picks.astype(jnp.bfloat16)
            cols = slice(turn * plane * capacity, (turn + 1) * plane * capacity)
            mix_high[q, :, cols] = high
            mix_low[q, :, cols] = (picks - high.astype(jnp.float32)).astype(jnp.bfloat16)

    def slot_copy(to):
        return remote(slots_out.at[to[2]], slots_in.at[spot], slot_send, slot_recv, to)

    normalize(0, tokens)
    pl.semaphore_wait(barrier, n - 1)
    for each in route_copies:
        each.start()
    token_copies[1].start()
    token_copies[0].start()

    early = 3 * n // 16
    loads[0].wait()
    loads[1].wait()
    cast_first(0)
    lax.fori_loop(0, early, send_first, 0)

    for each in route_copies:
        each.wait_recv()
    fill_slots(0, routes_t)
    token_copies[1].wait_recv()
    token_copies[2].start()
    lax.fori_loop(early, n // 2, send_first, 0)
    normalize(2, arrived.at[1])
    fill_slots(2, far_routes.at[1])
    token_copies[0].wait_recv()
    normalize(1, arrived.at[0])
    fill_slots(1, far_routes.at[0])
    cast_first(n // 2 + 1)
    lax.fori_loop(n // 2 + 1, n // 2 + n // 4, send_first, 0)
    token_copies[2].wait_recv()
    normalize(3, arrived.at[2])
    fill_slots(3, far_routes.at[2])

    def send_slots(step, carry):
        slot_copy(device(0, step)).start()
        return carry

    slots_in[spot] = slots_out[spot]
    lax.fori_loop(1, plane, send_slots, 0)
    lax.fori_loop(n // 2 + n // 4, n - 1, send_first, 0)
    first_copy(peer(n - 1)).start()

    me = fs * n_tp + tp
    mine_rows = pl.ds(pl.multiple_of(fs * tile_rows, tile_rows), tile_rows)
    mine_cols = pl.ds(pl.multiple_of(tp * tile_cols, tile_cols), tile_cols)
    in_mats[0, mine_rows, mine_cols] = in_tiles[me, 0]
    in_mats[1, mine_rows, mine_cols] = in_tiles[me, 1]

    loads[2].wait()
    cast_second(0)

    def send_second(step, carry):
        cast_second(step + 1)
        second_copy(0, peer(step)).start()
        return carry

    lax.fori_loop(0, n // 2, send_second, 0)
    out_mat[:, own_rows, own_lanes] = out_tiles[me]
    cast_second(n // 2 + 1)

    def send_near(step, carry):
        cast_second(step + 1)
        near_copy(peer(step)).start()
        return carry

    lax.fori_loop(n // 2 + 1, n - 1, send_near, 0)
    near_copy(peer(n - 1)).start()

    def send_chunk(c):
        def send_one(step, carry):
            second_copy(c, peer(step)).start()
            return carry

        lax.fori_loop(0, n // 2, send_one, 0)

    send_chunk(1)
    fill_mix(0, routes_t, weight_t)
    fill_mix(1, far_routes.at[1], far_weight)

    near = device(1, 0)

    def take(size_ref, send, recv):
        return remote(size_ref, size_ref, send, recv, near)

    slots_all = take(slots_in.at[pl.ds(0, plane - 1)], slot_send, slot_recv)
    first_all = take(in_tiles.at[pl.ds(0, n - 1)], first_send, first_recv)
    near_all = take(out_tiles.at[pl.ds(0, n // 2 - 1)], near_send, near_recv)

    def second_all(c):
        return take(out_tiles.at[pl.ds(0, n // 2), c], second_send.at[c], second_recv.at[c])

    def back_all(c):
        return take(
            rows_in.at[c, :, pl.ds(0, n // 2 - 1)], back_send.at[c], back_recv.at[c]
        )

    slots_all.wait_recv()
    first_all.wait_recv()
    stores = [
        pltpu.make_async_copy(in_mats.at[0], gate_out.at[0], store_sem.at[0]),
        pltpu.make_async_copy(in_mats.at[1], up_out.at[0], store_sem.at[1]),
    ]
    stores[0].start()
    stores[1].start()

    group = active.shape[1]
    held = group // (planes * capacity)

    def activate(g, carry):
        inputs = slots_in[pl.ds(g * held, held)].astype(jnp.float32)
        inputs = inputs.reshape(group, width).astype(jnp.bfloat16)
        gate_pre = jnp.dot(inputs, in_mats[0], preferred_element_type=jnp.float32)
        up_pre = jnp.dot(inputs, in_mats[1], preferred_element_type=jnp.float32)
        gate_part = jnp.minimum(gate_pre, clamp_limit)
        linear_part = jnp.clip(up_pre, -clamp_limit, clamp_limit)
        active[g] = (
            gate_part * jax.nn.sigmoid(sigmoid_slope * gate_part) * (linear_part + 1.0)
        ).astype(jnp.bfloat16)
        return carry

    lax.fori_loop(0, active.shape[0], activate, 0)
    near_all.wait_recv()

    def back_copy(c, turn, shift):
        to = device(turn, shift)
        return remote(
            rows_out.at[c, turn, to[2]],
            rows_in.at[c, :, turn * plane + spot],
            back_send.at[c],
            back_recv.at[c],
            to,
        )

    def store_down(c, k):
        return pltpu.make_async_copy(
            out_mat.at[c, :, k * lanes : (k + 1) * lanes],
            down_out.at[0, :, k * down_cols + c * lanes : k * down_cols + (c + 1) * lanes],
            store_sem.at[2 + c * n_tp + k],
        )

    def project(c):
        second_all(c).wait_recv()

        def project_group(g, carry):
            rows = jnp.dot(active[g], out_mat[c], preferred_element_type=jnp.float32)
            rows = rows.reshape(held, planes, capacity, block).astype(jnp.bfloat16)
            spots = pl.ds(g * held, held)
            for turn in range(2):
                for q in range(2):
                    rows_out[c, turn, spots, q] = rows[:, 2 * q + turn]
            return carry

        lax.fori_loop(0, active.shape[0], project_group, 0)
        for k in range(n_tp):
            store_down(c, k).start()

        def send_back(step, carry):
            back_copy(c, 1, step).start()
            return carry

        def send_side(step, carry):
            back_copy(c, 0, step).start()
            return carry

        lax.fori_loop(1, plane, send_side, 0)
        lax.fori_loop(0, plane, send_back, 0)
        for q in range(2):
            rows_in[c, q, spot] = rows_out[c, 0, spot, q]

    span = 2 * plane * capacity

    def combine(c, q):
        rows = rows_in[c, q].astype(jnp.float32).reshape(span, block).astype(jnp.bfloat16)
        total = jnp.dot(mix_high[q], rows, preferred_element_type=jnp.float32)
        return total + jnp.dot(mix_low[q], rows, preferred_element_type=jnp.float32)

    def part_copy(c):
        return remote(part_out.at[c], part_in.at[c], part_send.at[c], part_recv.at[c], device(2, 0))

    def give(c):
        back_all(c).wait_recv()
        part_out[c] = combine(c, 1).astype(jnp.bfloat16)

    def finish(c):
        total = combine(c, 0)
        part_copy(c).wait_recv()
        total = (total + part_in[c].astype(jnp.float32)).astype(jnp.bfloat16)
        for k in range(n_tp):
            start = k * down_cols + c * lanes
            mixed[:, start : start + lanes] = total[:, k * lanes : (k + 1) * lanes]

    for c in range(chunks):
        project(c)
        if c + 2 < chunks:
            send_chunk(c + 2)
        if c > 0:
            give(c - 1)
            part_copy(c - 1).start()
    give(chunks - 1)
    part_copy(chunks - 1).start()
    for c in range(chunks):
        finish(c)

    first_all.wait_send()
    near_all.wait_send()
    slots_all.wait_send()
    for c in range(chunks):
        second_all(c).wait_send()
        back_all(c).wait_send()
        part_copy(c).wait_send()
    for each in token_copies + route_copies:
        each.wait_send()
    for store in stores:
        store.wait()
    for c in range(chunks):
        for k in range(n_tp):
            store_down(c, k).wait()


def direct_shards(
    tokens, routes, route_weight, norm_gain, gate_weight, up_weight, down_weight
):
    n_fs, n_tp = lax.axis_size("fs"), lax.axis_size("tp")
    n = n_fs * n_tp
    tok_rows, width = tokens.shape
    tile_rows, tile_cols = gate_weight.shape[1:]
    down_rows, down_cols = down_weight.shape[1:]
    hidden = n_tp * tile_cols
    lanes = 128
    chunks = down_cols // lanes
    block = n_tp * lanes
    plane = n // 4
    per_token = routes.shape[1]
    capacity = max(2, 3 * tok_rows * per_token // (2 * n))
    bf16, f32 = jnp.bfloat16, jnp.float32
    whole = pl.BlockSpec(memory_space=pltpu.VMEM)
    apart = pl.BlockSpec(memory_space=pl.ANY)
    dma = pltpu.SemaphoreType.DMA
    groups = 4
    return pl.pallas_call(
        functools.partial(exchange_kernel, (n_fs, n_tp, capacity)),
        out_shape=(
            jax.ShapeDtypeStruct((1, width, hidden), bf16),
            jax.ShapeDtypeStruct((1, width, hidden), bf16),
            jax.ShapeDtypeStruct((1, hidden, width), bf16),
            jax.ShapeDtypeStruct((tok_rows, width), bf16),
        ),
        in_specs=[whole] * 4 + [apart] * 3,
        out_specs=(apart, apart, apart, whole),
        scratch_shapes=[
            pltpu.VMEM((n, tile_rows, tile_cols), f32),
            pltpu.VMEM((n, tile_rows, tile_cols), f32),
            pltpu.VMEM((n, down_rows, down_cols), f32),
            pltpu.VMEM((tile_rows, tile_cols), f32),
            pltpu.VMEM((n, 2, tile_rows, tile_cols), bf16),
            pltpu.VMEM((n, chunks, down_rows, lanes), bf16),
            pltpu.VMEM((2, width, hidden), bf16),
            pltpu.VMEM((chunks, hidden, block), bf16),
            pltpu.VMEM((3, tok_rows, width), bf16),
            pltpu.VMEM((4, tok_rows, width), bf16),
            pltpu.VMEM((plane, 4, capacity, width), bf16),
            pltpu.VMEM((plane, 4, capacity, width), bf16),
            pltpu.VMEM((groups, n * capacity // groups, hidden), bf16),
            pltpu.VMEM((3, per_token, tok_rows), routes.dtype),
            pltpu.VMEM((per_token, tok_rows), f32),
            pltpu.VMEM((2, tok_rows, 2 * plane * capacity), bf16),
            pltpu.VMEM((2, tok_rows, 2 * plane * capacity), bf16),
            pltpu.VMEM((chunks, 2, plane, 2, capacity, block), bf16),
            pltpu.VMEM((chunks, 2, 2 * plane, capacity, block), bf16),
            pltpu.VMEM((chunks, tok_rows, block), bf16),
            pltpu.VMEM((chunks, tok_rows, block), bf16),
            dma((3,)),
            dma((2 + chunks * n_tp,)),
            dma((3,)),
            dma((3,)),
            dma((4,)),
            dma((4,)),
            dma,
            dma,
            dma,
            dma,
            dma,
            dma,
        ]
        + [dma((chunks,))] * 6,
        compiler_params=pltpu.CompilerParams(
            collective_id=0, has_side_effects=True, vmem_limit_bytes=60 * 1024 * 1024
        ),
    )(
        tokens,
        routes.T,
        route_weight.T,
        norm_gain.reshape(tile_rows // lanes, lanes),
        gate_weight,
        up_weight,
        down_weight,
    )


def aligned(mesh, tokens, routes, gate_weight, down_weight):
    n_fs, n_tp = mesh.shape["fs"], mesh.shape["tp"]
    n = n_fs * n_tp
    tok_rows = tokens.shape[0] // n
    capacity = max(2, 3 * tok_rows * routes.shape[1] // (2 * n))
    return (
        gate_weight.shape[0] == n
        and n_fs % 4 == 0
        and n % 32 == 0
        and capacity % 8 == 0
        and tok_rows % 128 == 0
        and tokens.shape[1] % 512 == 0
        and gate_weight.shape[1] // n_fs % 128 == 0
        and gate_weight.shape[2] // n_tp % 128 == 0
        and down_weight.shape[1] // n_fs % 16 == 0
        and down_weight.shape[2] // n_tp % 128 == 0
    )


def solution(mesh):
    placed = (
        P(("fs", "tp"), None),
        P(("fs", "tp"), None),
        P(("fs", "tp"), None),
        P("fs"),
        P(None, "fs", "tp"),
        P(None, "fs", "tp"),
        P(None, "fs", "tp"),
    )

    def run(tokens, routes, route_weight, norm_gain, gate_weight, up_weight, down_weight):
        direct = aligned(mesh, tokens, routes, gate_weight, down_weight)
        return jax.shard_map(
            direct_shards if direct else shards,
            mesh=mesh,
            in_specs=placed,
            out_specs=(
                P(("fs", "tp"), None, None),
                P(("fs", "tp"), None, None),
                P(("fs", "tp"), None, None),
                P(("fs", "tp"), None),
            ),
            check_vma=False,
        )(tokens, routes, route_weight, norm_gain, gate_weight, up_weight, down_weight)

    return run
```

```python
import functools

import jax
import jax.numpy as jnp
from jax import lax
from jax.experimental import pallas as pl
from jax.experimental.pallas import tpu as pltpu
from jax.sharding import PartitionSpec as P

norm_epsilon = 1e-06
clamp_limit = 7.0
sigmoid_slope = 1.702
MESH = pl.DeviceIdType.MESH


def feed(inputs, gate_mat, up_mat, down_mat):
    gate_pre = jnp.dot(inputs, gate_mat, preferred_element_type=jnp.float32)
    up_pre = jnp.dot(inputs, up_mat, preferred_element_type=jnp.float32)
    gate_part = jnp.minimum(gate_pre, clamp_limit)
    linear_part = jnp.clip(up_pre, -clamp_limit, clamp_limit)
    activation = (
        gate_part * jax.nn.sigmoid(sigmoid_slope * gate_part) * (linear_part + 1.0)
    ).astype(jnp.bfloat16)
    return jnp.dot(activation, down_mat, preferred_element_type=jnp.float32).astype(jnp.bfloat16)


def assemble(received, rows_groups, column_groups):
    tile_rows = received.shape[2]
    tile_columns = received.shape[3]
    sources = received.reshape(rows_groups, column_groups, tile_rows, tile_columns)
    return sources.transpose(0, 2, 1, 3).reshape(
        1, rows_groups * tile_rows, column_groups * tile_columns
    )


def shards(tokens, routes, route_weight, norm_gain, gate_weight, up_weight, down_weight):
    gain_column = norm_gain[None, :, None]
    gate_tiles = (gate_weight * gain_column).astype(jnp.bfloat16)
    up_tiles = (up_weight * gain_column).astype(jnp.bfloat16)
    down_tiles = down_weight.astype(jnp.bfloat16)
    rows_groups = lax.axis_size("fs")
    column_groups = lax.axis_size("tp")
    arrived = (
        lax.all_to_all(gate_tiles[:, None], ("fs", "tp"), split_axis=0, concat_axis=1, tiled=True),
        lax.all_to_all(up_tiles[:, None], ("fs", "tp"), split_axis=0, concat_axis=1, tiled=True),
        lax.all_to_all(down_tiles[:, None], ("fs", "tp"), split_axis=0, concat_axis=1, tiled=True),
    )
    gate_new = assemble(arrived[0], rows_groups, column_groups)
    up_new = assemble(arrived[1], rows_groups, column_groups)
    down_new = assemble(arrived[2], rows_groups, column_groups)
    experts = rows_groups * column_groups
    tok_rows, model_width = tokens.shape
    per_token = routes.shape[1]
    capacity = max(2, 3 * tok_rows * per_token // (2 * experts))
    values = tokens.astype(jnp.float32)
    squares = jnp.mean(values * values, axis=1, keepdims=True)
    normed = (values * lax.rsqrt(squares + norm_epsilon)).astype(jnp.bfloat16)
    flat_routes = routes.reshape(-1)
    onehot = (flat_routes[:, None] == jnp.arange(experts, dtype=jnp.int32)[None, :]).astype(
        jnp.int32
    )
    earlier = jnp.cumsum(onehot, axis=0) - onehot
    rank = jnp.sum(earlier * onehot, axis=1)
    slot_index = flat_routes * capacity + rank
    slot_numbers = jnp.arange(experts * capacity, dtype=jnp.int32)
    select = jnp.any(
        slot_index.reshape(tok_rows, per_token)[None, :, :] == slot_numbers[:, None, None], axis=2
    )
    buffer = jnp.dot(
        select.astype(jnp.bfloat16), normed, preferred_element_type=jnp.float32
    ).astype(jnp.bfloat16)
    buffer = buffer.reshape(experts, 1, capacity, model_width)
    slot_rows = lax.all_to_all(buffer, ("fs", "tp"), split_axis=0, concat_axis=1, tiled=True)
    sources = slot_rows.shape[1]
    count = slot_rows.shape[2]
    expert_out = feed(slot_rows.reshape(-1, model_width), gate_new[0], up_new[0], down_new[0])
    expert_out = expert_out.reshape(1, sources, count, model_width)
    returned = lax.all_to_all(expert_out, ("fs", "tp"), split_axis=1, concat_axis=0, tiled=True)
    returned = returned.reshape(experts * capacity, model_width)
    picked = returned[slot_index].reshape(tok_rows, per_token, model_width)
    mixed = jnp.sum(picked.astype(jnp.float32) * route_weight[:, :, None], axis=1).astype(
        jnp.bfloat16
    )
    return (gate_new, up_new, down_new, mixed)


def exchange_kernel(
    sizes, tokens_far, routes_far, weight_far, gain_far, gate, up, down,
    in_mats, out_mat, mixed,
    tokens, routes_t, weight_t, gain, gate_in, up_in, down_in, gains, in_tiles, out_tiles,
    arrived, normed, slots_out, slots_in, active, far_routes, far_weight,
    mix_high, mix_low, rows_out, rows_in, part_out, part_in,
    load_sem, token_send, token_recv, route_send, route_recv,
    first_send, first_recv, near_send, near_recv, slot_send, slot_recv,
    second_send, second_recv, back_send, back_recv, part_send, part_recv,
):
    n_fs, n_tp, capacity = sizes
    n = n_fs * n_tp
    fs, tp = lax.axis_index("fs"), lax.axis_index("tp")
    tok_rows, width = tokens.shape
    tile_rows, tile_cols = gate_in.shape[1:]
    chunks, down_rows, lanes = out_tiles.shape[1:]
    down_cols = chunks * lanes
    block = n_tp * lanes
    per_token = routes_t.shape[0]

    planes = 4
    plane_fs = n_fs // planes
    plane = n // planes
    layer, place = fs // plane_fs, lax.rem(fs, plane_fs)
    spot = place * n_tp + tp

    def flip(turn):
        low = lax.rem(layer + turn, 2)
        high = lax.rem(layer // 2 + turn // 2, 2)
        return 2 * high + low

    def device(turn, shift):
        to_place = lax.rem(place + shift // n_tp, plane_fs)
        to_tp = lax.rem(tp + lax.rem(shift, n_tp), n_tp)
        return flip(turn) * plane_fs + to_place, to_tp, to_place * n_tp + to_tp

    def peer(step):
        crossing = 1 - lax.rem(step, 2)
        at = lax.rem(step // 2 + 1 - crossing, n // 2)
        to_fs, to_tp, _ = device(2 * crossing + lax.rem(at, 2), at // 2)
        return to_fs, to_tp, to_fs * n_tp + to_tp

    def remote(source, target, send, recv, to):
        return pltpu.make_async_remote_copy(
            src_ref=source,
            dst_ref=target,
            send_sem=send,
            recv_sem=recv,
            device_id=(to[0], to[1]),
            device_id_type=MESH,
        )

    barrier = pltpu.get_barrier_semaphore()

    def greet(step, carry):
        to = peer(step)
        pl.semaphore_signal(barrier, inc=1, device_id=(to[0], to[1]), device_id_type=MESH)
        return carry

    loads = [
        pltpu.make_async_copy(source, target, load_sem.at[i])
        for i, (source, target) in enumerate(
            [
                (gain_far, gain),
                (routes_far, routes_t),
                (weight_far, weight_t),
                (tokens_far, tokens),
                (gate, gate_in),
                (up, up_in),
                (down, down_in),
            ]
        )
    ]
    for load in loads:
        load.start()
    lax.fori_loop(0, n - 1, greet, 0)

    for load in loads[:4]:
        load.wait()
    for i in range(tile_rows // lanes):
        gains[i * lanes : (i + 1) * lanes, :] = jnp.transpose(
            jnp.broadcast_to(gain[i : i + 1, :], (tile_cols, lanes))
        )

    def token_copy(turn, source):
        to = 1 if turn == 3 else turn
        return remote(
            source, arrived.at[turn - 1], token_send.at[turn - 1], token_recv.at[turn - 1], device(to, 0)
        )

    def route_copy(turn):
        return remote(
            routes_t, far_routes.at[turn - 1], route_send.at[turn - 1], route_recv.at[turn - 1], device(turn, 0)
        )

    weight_copy = remote(weight_t, far_weight, route_send.at[3], route_recv.at[3], device(2, 0))
    token_copies = [
        token_copy(1, tokens),
        token_copy(2, tokens),
        token_copy(3, arrived.at[1]),
    ]
    route_copies = [route_copy(1), route_copy(2), route_copy(3), weight_copy]

    def first_copy(to):
        return remote(
            in_tiles.at[to[2]],
            in_mats.at[
                :,
                pl.ds(pl.multiple_of(fs * tile_rows, tile_rows), tile_rows),
                pl.ds(pl.multiple_of(tp * tile_cols, tile_cols), tile_cols),
            ],
            first_send,
            first_recv,
            to,
        )

    own_rows = pl.ds(pl.multiple_of(fs * down_rows, down_rows), down_rows)
    own_lanes = pl.ds(pl.multiple_of(tp * lanes, lanes), lanes)

    def near_copy(to):
        return remote(
            out_tiles.at[to[2]], out_mat.at[:, own_rows, own_lanes], near_send, near_recv, to
        )

    def second_copy(c, to):
        return remote(
            out_tiles.at[to[2], c],
            out_mat.at[c, own_rows, own_lanes],
            second_send.at[c],
            second_recv.at[c],
            to,
        )

    def cast_first(step):
        e = peer(step)[2]
        in_tiles[e, 0] = (gate_in[e] * gains[...]).astype(jnp.bfloat16)
        in_tiles[e, 1] = (up_in[e] * gains[...]).astype(jnp.bfloat16)

    def cast_second(step):
        e = peer(step)[2]
        for c in range(chunks):
            out_tiles[e, c] = down_in[e, :, c * lanes : (c + 1) * lanes].astype(jnp.bfloat16)

    def send_first(step, carry):
        cast_first(step + 1)
        first_copy(peer(step)).start()
        return carry

    before = (
        lax.broadcasted_iota(jnp.int32, (tok_rows, tok_rows), 0)
        < lax.broadcasted_iota(jnp.int32, (tok_rows, tok_rows), 1)
    ).astype(jnp.float32).astype(jnp.bfloat16)

    def named_in(turn, paths, shares):
        experts = lax.broadcasted_iota(jnp.int32, (plane, tok_rows), 0) + flip(turn) * plane
        named = jnp.zeros((plane, tok_rows), jnp.float32)
        scaled = jnp.zeros((plane, tok_rows), jnp.float32)
        for k in range(per_token):
            hit = paths[k : k + 1, :] == experts
            named = named + hit.astype(jnp.float32)
            if shares is not None:
                scaled = scaled + jnp.where(hit, shares[k : k + 1, :], 0.0)
        rank = jnp.dot(named.astype(jnp.bfloat16), before, preferred_element_type=jnp.float32)
        rank = jnp.where(named > 0.5, rank, -1.0)
        number = lax.broadcasted_iota(jnp.int32, (plane, capacity, tok_rows), 1).astype(jnp.float32)
        return (rank[:, None, :] == number).astype(jnp.float32), scaled

    def normalize(turn, rows_ref):
        values = rows_ref[...].astype(jnp.float32)
        squares = jnp.mean(values * values, axis=1, keepdims=True)
        normed[turn] = (values * lax.rsqrt(squares + norm_epsilon)).astype(jnp.bfloat16)

    def fill_slots(turn, paths):
        select, _ = named_in(0, paths, None)
        rows = jnp.dot(
            select.reshape(plane * capacity, tok_rows).astype(jnp.bfloat16),
            normed[turn],
            preferred_element_type=jnp.float32,
        )
        slots_out[:, turn] = rows.reshape(plane, capacity, width).astype(jnp.bfloat16)

    def fill_mix(q, paths, shares):
        for turn in range(2):
            select, scaled = named_in(turn, paths, shares)
            picks = jnp.transpose(
                (select * scaled[:, None, :]).reshape(plane * capacity, tok_rows)
            )
            high = picks.astype(jnp.bfloat16)
            cols = slice(turn * plane * capacity, (turn + 1) * plane * capacity)
            mix_high[q, :, cols] = high
            mix_low[q, :, cols] = (picks - high.astype(jnp.float32)).astype(jnp.bfloat16)

    def slot_copy(turn, to):
        return remote(
            slots_out.at[to[2], turn], slots_in.at[spot, turn], slot_send, slot_recv, to
        )

    def send_slots(turn):
        def send_one(step, carry):
            slot_copy(turn, device(0, step)).start()
            return carry

        lax.fori_loop(1, plane, send_one, 0)
        slots_in[spot, turn] = slots_out[spot, turn]

    def send_some(start, stop):
        lax.fori_loop(start, stop, send_first, 0)

    normalize(0, tokens)
    pl.semaphore_wait(barrier, n - 1)
    for each in route_copies:
        each.start()
    token_copies[1].start()
    token_copies[0].start()
    fill_slots(0, routes_t)
    loads[4].wait()
    loads[5].wait()
    cast_first(0)
    send_some(0, n // 8)
    send_slots(0)
    send_some(n // 8, 3 * n // 8)
    for each in route_copies:
        each.wait_recv()
    token_copies[1].wait_recv()
    token_copies[2].start()
    normalize(2, arrived.at[1])
    fill_slots(2, far_routes.at[1])
    send_some(3 * n // 8, n // 2)
    send_slots(2)
    token_copies[0].wait_recv()
    normalize(1, arrived.at[0])
    fill_slots(1, far_routes.at[0])
    send_some(n // 2, 5 * n // 8)
    send_slots(1)
    token_copies[2].wait_recv()
    normalize(3, arrived.at[2])
    fill_slots(3, far_routes.at[2])
    send_some(5 * n // 8, 6 * n // 8)
    send_slots(3)
    send_some(6 * n // 8, n - 1)

    me = fs * n_tp + tp
    mine_rows = pl.ds(pl.multiple_of(fs * tile_rows, tile_rows), tile_rows)
    mine_cols = pl.ds(pl.multiple_of(tp * tile_cols, tile_cols), tile_cols)
    in_mats[0, mine_rows, mine_cols] = in_tiles[me, 0]
    in_mats[1, mine_rows, mine_cols] = in_tiles[me, 1]

    loads[6].wait()
    cast_second(0)
    cast_second(1)

    def send_second(step, carry):
        cast_second(2 * step + 2)
        second_copy(0, peer(2 * step)).start()
        cast_second(2 * step + 3)
        near_copy(peer(2 * step + 1)).start()
        return carry

    lax.fori_loop(0, n // 2 - 1, send_second, 0)
    second_copy(0, peer(n - 2)).start()
    out_mat[:, own_rows, own_lanes] = out_tiles[me]

    def send_chunk(c):
        def send_one(step, carry):
            second_copy(c, peer(2 * step)).start()
            return carry

        lax.fori_loop(0, n // 2, send_one, 0)

    send_chunk(1)
    fill_mix(0, routes_t, weight_t)
    fill_mix(1, far_routes.at[1], far_weight)

    near = device(1, 0)

    def take(size_ref, send, recv):
        return remote(size_ref, size_ref, send, recv, near)

    slots_all = take(slots_in.at[pl.ds(0, plane - 1)], slot_send, slot_recv)
    first_all = take(in_tiles.at[pl.ds(0, n - 1)], first_send, first_recv)
    near_all = take(out_tiles.at[pl.ds(0, n // 2 - 1)], near_send, near_recv)

    def second_all(c):
        return take(out_tiles.at[pl.ds(0, n // 2), c], second_send.at[c], second_recv.at[c])

    def back_all(c):
        return take(
            rows_in.at[c, :, pl.ds(0, n // 2 - 1)], back_send.at[c], back_recv.at[c]
        )

    slots_all.wait_recv()
    first_all.wait_recv()

    group = active.shape[1]
    held = group // (planes * capacity)

    def activate(g, carry):
        inputs = slots_in[pl.ds(g * held, held)].astype(jnp.float32)
        inputs = inputs.reshape(group, width).astype(jnp.bfloat16)
        gate_pre = jnp.dot(inputs, in_mats[0], preferred_element_type=jnp.float32)
        up_pre = jnp.dot(inputs, in_mats[1], preferred_element_type=jnp.float32)
        gate_part = jnp.minimum(gate_pre, clamp_limit)
        linear_part = jnp.clip(up_pre, -clamp_limit, clamp_limit)
        active[g] = (
            gate_part * jax.nn.sigmoid(sigmoid_slope * gate_part) * (linear_part + 1.0)
        ).astype(jnp.bfloat16)
        return carry

    lax.fori_loop(0, active.shape[0], activate, 0)
    near_all.wait_recv()

    def back_copy(c, turn, shift):
        to = device(turn, shift)
        return remote(
            rows_out.at[c, turn, to[2]],
            rows_in.at[c, :, turn * plane + spot],
            back_send.at[c],
            back_recv.at[c],
            to,
        )

    def project(c):
        second_all(c).wait_recv()

        def project_group(g, carry):
            rows = jnp.dot(active[g], out_mat[c], preferred_element_type=jnp.float32)
            rows = rows.reshape(held, planes, capacity, block).astype(jnp.bfloat16)
            spots = pl.ds(g * held, held)
            for turn in range(2):
                for q in range(2):
                    rows_out[c, turn, spots, q] = rows[:, 2 * q + turn]
            return carry

        lax.fori_loop(0, active.shape[0], project_group, 0)

        def send_back(step, carry):
            back_copy(c, 1, step).start()
            return carry

        def send_side(step, carry):
            back_copy(c, 0, step).start()
            return carry

        lax.fori_loop(1, plane, send_side, 0)
        lax.fori_loop(0, plane, send_back, 0)
        for q in range(2):
            rows_in[c, q, spot] = rows_out[c, 0, spot, q]

    span = 2 * plane * capacity

    def combine(c, q):
        rows = rows_in[c, q].astype(jnp.float32).reshape(span, block).astype(jnp.bfloat16)
        total = jnp.dot(mix_high[q], rows, preferred_element_type=jnp.float32)
        return total + jnp.dot(mix_low[q], rows, preferred_element_type=jnp.float32)

    def part_copy(c):
        return remote(part_out.at[c], part_in.at[c], part_send.at[c], part_recv.at[c], device(2, 0))

    def give(c):
        back_all(c).wait_recv()
        part_out[c] = combine(c, 1).astype(jnp.bfloat16)

    def finish(c):
        total = combine(c, 0)
        part_copy(c).wait_recv()
        total = (total + part_in[c].astype(jnp.float32)).astype(jnp.bfloat16)
        for k in range(n_tp):
            start = k * down_cols + c * lanes
            mixed[:, start : start + lanes] = total[:, k * lanes : (k + 1) * lanes]

    for c in range(chunks):
        project(c)
        if c + 2 < chunks:
            send_chunk(c + 2)
        if c > 0:
            give(c - 1)
            part_copy(c - 1).start()
    give(chunks - 1)
    part_copy(chunks - 1).start()
    for c in range(chunks):
        finish(c)

    first_all.wait_send()
    near_all.wait_send()
    slots_all.wait_send()
    for c in range(chunks):
        second_all(c).wait_send()
        back_all(c).wait_send()
        part_copy(c).wait_send()
    for each in token_copies + route_copies:
        each.wait_send()


def keep_kernel(in_mats, out_mat, rows, gate_out, up_out, down_out, mixed, sem):
    chunks, _, block = out_mat.shape
    n_tp = block // 128
    lanes = block // n_tp
    down_cols = chunks * lanes
    copies = [
        (in_mats.at[0], gate_out.at[0]),
        (in_mats.at[1], up_out.at[0]),
        (rows, mixed),
    ]
    for c in range(chunks):
        for k in range(n_tp):
            start = k * down_cols + c * lanes
            copies.append(
                (
                    out_mat.at[c, :, k * lanes : (k + 1) * lanes],
                    down_out.at[0, :, start : start + lanes],
                )
            )
    copies = [
        pltpu.make_async_copy(source, target, sem.at[i])
        for i, (source, target) in enumerate(copies)
    ]
    for copy in copies:
        copy.start()
    for copy in copies:
        copy.wait()


def direct_shards(
    tokens, routes, route_weight, norm_gain, gate_weight, up_weight, down_weight
):
    n_fs, n_tp = lax.axis_size("fs"), lax.axis_size("tp")
    n = n_fs * n_tp
    tok_rows, width = tokens.shape
    tile_rows, tile_cols = gate_weight.shape[1:]
    down_rows, down_cols = down_weight.shape[1:]
    hidden = n_tp * tile_cols
    lanes = 128
    chunks = down_cols // lanes
    block = n_tp * lanes
    plane = n // 4
    per_token = routes.shape[1]
    capacity = max(2, 3 * tok_rows * per_token // (2 * n))
    bf16, f32 = jnp.bfloat16, jnp.float32
    whole = pl.BlockSpec(memory_space=pltpu.VMEM)
    apart = pl.BlockSpec(memory_space=pltpu.HBM)
    dma = pltpu.SemaphoreType.DMA
    groups = 4
    in_mats, out_mat, rows = pl.pallas_call(
        functools.partial(exchange_kernel, (n_fs, n_tp, capacity)),
        out_shape=(
            pltpu.VMEM((2, width, hidden), bf16),
            pltpu.VMEM((chunks, hidden, block), bf16),
            pltpu.VMEM((tok_rows, width), bf16),
        ),
        in_specs=[apart] * 7,
        out_specs=(whole, whole, whole),
        scratch_shapes=[
            pltpu.VMEM((tok_rows, width), tokens.dtype),
            pltpu.VMEM((per_token, tok_rows), routes.dtype),
            pltpu.VMEM((per_token, tok_rows), f32),
            pltpu.VMEM((tile_rows // lanes, lanes), f32),
            pltpu.VMEM((n, tile_rows, tile_cols), f32),
            pltpu.VMEM((n, tile_rows, tile_cols), f32),
            pltpu.VMEM((n, down_rows, down_cols), f32),
            pltpu.VMEM((tile_rows, tile_cols), f32),
            pltpu.VMEM((n, 2, tile_rows, tile_cols), bf16),
            pltpu.VMEM((n, chunks, down_rows, lanes), bf16),
            pltpu.VMEM((3, tok_rows, width), bf16),
            pltpu.VMEM((4, tok_rows, width), bf16),
            pltpu.VMEM((plane, 4, capacity, width), bf16),
            pltpu.VMEM((plane, 4, capacity, width), bf16),
            pltpu.VMEM((groups, n * capacity // groups, hidden), bf16),
            pltpu.VMEM((3, per_token, tok_rows), routes.dtype),
            pltpu.VMEM((per_token, tok_rows), f32),
            pltpu.VMEM((2, tok_rows, 2 * plane * capacity), bf16),
            pltpu.VMEM((2, tok_rows, 2 * plane * capacity), bf16),
            pltpu.VMEM((chunks, 2, plane, 2, capacity, block), bf16),
            pltpu.VMEM((chunks, 2, 2 * plane, capacity, block), bf16),
            pltpu.VMEM((chunks, tok_rows, block), bf16),
            pltpu.VMEM((chunks, tok_rows, block), bf16),
            dma((7,)),
            dma((3,)),
            dma((3,)),
            dma((4,)),
            dma((4,)),
            dma,
            dma,
            dma,
            dma,
            dma,
            dma,
        ]
        + [dma((chunks,))] * 6,
        compiler_params=pltpu.CompilerParams(
            collective_id=0, has_side_effects=True, vmem_limit_bytes=50 * 1024 * 1024
        ),
    )(
        tokens,
        routes.T,
        route_weight.T,
        norm_gain.reshape(tile_rows // lanes, lanes),
        gate_weight,
        up_weight,
        down_weight,
    )
    return pl.pallas_call(
        keep_kernel,
        out_shape=(
            jax.ShapeDtypeStruct((1, width, hidden), bf16),
            jax.ShapeDtypeStruct((1, width, hidden), bf16),
            jax.ShapeDtypeStruct((1, hidden, width), bf16),
            jax.ShapeDtypeStruct((tok_rows, width), bf16),
        ),
        in_specs=[whole] * 3,
        out_specs=(apart,) * 4,
        scratch_shapes=[dma((3 + chunks * n_tp,))],
        compiler_params=pltpu.CompilerParams(vmem_limit_bytes=8 * 1024 * 1024),
    )(in_mats, out_mat, rows)


def aligned(mesh, tokens, routes, gate_weight, down_weight):
    n_fs, n_tp = mesh.shape["fs"], mesh.shape["tp"]
    n = n_fs * n_tp
    tok_rows = tokens.shape[0] // n
    capacity = max(2, 3 * tok_rows * routes.shape[1] // (2 * n))
    return (
        gate_weight.shape[0] == n
        and n_fs % 4 == 0
        and n % 32 == 0
        and capacity % 8 == 0
        and tok_rows % 128 == 0
        and tokens.shape[1] % 512 == 0
        and gate_weight.shape[1] // n_fs % 128 == 0
        and gate_weight.shape[2] // n_tp % 128 == 0
        and down_weight.shape[1] // n_fs % 16 == 0
        and down_weight.shape[2] // n_tp % 128 == 0
    )


def solution(mesh):
    placed = (
        P(("fs", "tp"), None),
        P(("fs", "tp"), None),
        P(("fs", "tp"), None),
        P("fs"),
        P(None, "fs", "tp"),
        P(None, "fs", "tp"),
        P(None, "fs", "tp"),
    )

    def run(tokens, routes, route_weight, norm_gain, gate_weight, up_weight, down_weight):
        direct = aligned(mesh, tokens, routes, gate_weight, down_weight)
        return jax.shard_map(
            direct_shards if direct else shards,
            mesh=mesh,
            in_specs=placed,
            out_specs=(
                P(("fs", "tp"), None, None),
                P(("fs", "tp"), None, None),
                P(("fs", "tp"), None, None),
                P(("fs", "tp"), None),
            ),
            check_vma=False,
        )(tokens, routes, route_weight, norm_gain, gate_weight, up_weight, down_weight)

    return run
```

```python
import functools

import jax
import jax.numpy as jnp
from jax import lax
from jax.experimental import pallas as pl
from jax.experimental.pallas import tpu as pltpu
from jax.sharding import PartitionSpec as P

norm_epsilon = 1e-06
clamp_limit = 7.0
sigmoid_slope = 1.702
MESH = pl.DeviceIdType.MESH


def feed(inputs, gate_mat, up_mat, down_mat):
    gate_pre = jnp.dot(inputs, gate_mat, preferred_element_type=jnp.float32)
    up_pre = jnp.dot(inputs, up_mat, preferred_element_type=jnp.float32)
    gate_part = jnp.minimum(gate_pre, clamp_limit)
    linear_part = jnp.clip(up_pre, -clamp_limit, clamp_limit)
    activation = (
        gate_part * jax.nn.sigmoid(sigmoid_slope * gate_part) * (linear_part + 1.0)
    ).astype(jnp.bfloat16)
    return jnp.dot(activation, down_mat, preferred_element_type=jnp.float32).astype(jnp.bfloat16)


def assemble(received, rows_groups, column_groups):
    tile_rows = received.shape[2]
    tile_columns = received.shape[3]
    sources = received.reshape(rows_groups, column_groups, tile_rows, tile_columns)
    return sources.transpose(0, 2, 1, 3).reshape(
        1, rows_groups * tile_rows, column_groups * tile_columns
    )


def shards(tokens, routes, route_weight, norm_gain, gate_weight, up_weight, down_weight):
    gain_column = norm_gain[None, :, None]
    gate_tiles = (gate_weight * gain_column).astype(jnp.bfloat16)
    up_tiles = (up_weight * gain_column).astype(jnp.bfloat16)
    down_tiles = down_weight.astype(jnp.bfloat16)
    rows_groups = lax.axis_size("fs")
    column_groups = lax.axis_size("tp")
    arrived = (
        lax.all_to_all(gate_tiles[:, None], ("fs", "tp"), split_axis=0, concat_axis=1, tiled=True),
        lax.all_to_all(up_tiles[:, None], ("fs", "tp"), split_axis=0, concat_axis=1, tiled=True),
        lax.all_to_all(down_tiles[:, None], ("fs", "tp"), split_axis=0, concat_axis=1, tiled=True),
    )
    gate_new = assemble(arrived[0], rows_groups, column_groups)
    up_new = assemble(arrived[1], rows_groups, column_groups)
    down_new = assemble(arrived[2], rows_groups, column_groups)
    experts = rows_groups * column_groups
    tok_rows, model_width = tokens.shape
    per_token = routes.shape[1]
    capacity = max(2, 3 * tok_rows * per_token // (2 * experts))
    values = tokens.astype(jnp.float32)
    squares = jnp.mean(values * values, axis=1, keepdims=True)
    normed = (values * lax.rsqrt(squares + norm_epsilon)).astype(jnp.bfloat16)
    flat_routes = routes.reshape(-1)
    onehot = (flat_routes[:, None] == jnp.arange(experts, dtype=jnp.int32)[None, :]).astype(
        jnp.int32
    )
    earlier = jnp.cumsum(onehot, axis=0) - onehot
    rank = jnp.sum(earlier * onehot, axis=1)
    slot_index = flat_routes * capacity + rank
    slot_numbers = jnp.arange(experts * capacity, dtype=jnp.int32)
    select = jnp.any(
        slot_index.reshape(tok_rows, per_token)[None, :, :] == slot_numbers[:, None, None], axis=2
    )
    buffer = jnp.dot(
        select.astype(jnp.bfloat16), normed, preferred_element_type=jnp.float32
    ).astype(jnp.bfloat16)
    buffer = buffer.reshape(experts, 1, capacity, model_width)
    slot_rows = lax.all_to_all(buffer, ("fs", "tp"), split_axis=0, concat_axis=1, tiled=True)
    sources = slot_rows.shape[1]
    count = slot_rows.shape[2]
    expert_out = feed(slot_rows.reshape(-1, model_width), gate_new[0], up_new[0], down_new[0])
    expert_out = expert_out.reshape(1, sources, count, model_width)
    returned = lax.all_to_all(expert_out, ("fs", "tp"), split_axis=1, concat_axis=0, tiled=True)
    returned = returned.reshape(experts * capacity, model_width)
    picked = returned[slot_index].reshape(tok_rows, per_token, model_width)
    mixed = jnp.sum(picked.astype(jnp.float32) * route_weight[:, :, None], axis=1).astype(
        jnp.bfloat16
    )
    return (gate_new, up_new, down_new, mixed)


def exchange_kernel(
    sizes, tokens_far, routes_far, weight_far, gain_far, gate, up, down,
    in_mats, out_mat, mixed,
    tokens, routes_t, weight_t, gain, gate_in, up_in, down_in, gains, in_tiles, out_tiles,
    arrived, normed, slots_out, slots_in, active, far_routes, far_weight,
    mix_high, mix_low, rows_out, rows_in, side_out, side_in, totals, part_out, part_in,
    load_sem, token_send, token_recv, route_send, route_recv,
    first_send, first_recv, near_send, near_recv, slot_send, slot_recv,
    second_send, second_recv, back_send, back_recv, side_send, side_recv, part_send, part_recv,
):
    n_fs, n_tp, capacity = sizes
    n = n_fs * n_tp
    fs, tp = lax.axis_index("fs"), lax.axis_index("tp")
    tok_rows, width = tokens.shape
    tile_rows, tile_cols = gate_in.shape[1:]
    chunks, down_rows, lanes = out_tiles.shape[1:]
    down_cols = chunks * lanes
    block = n_tp * lanes
    per_token = routes_t.shape[0]

    planes = 4
    plane_fs = n_fs // planes
    plane = n // planes
    layer, place = fs // plane_fs, lax.rem(fs, plane_fs)
    spot = place * n_tp + tp

    def flip(turn):
        low = lax.rem(layer + turn, 2)
        high = lax.rem(layer // 2 + turn // 2, 2)
        return 2 * high + low

    def device(turn, shift):
        to_place = lax.rem(place + shift // n_tp, plane_fs)
        to_tp = lax.rem(tp + lax.rem(shift, n_tp), n_tp)
        return flip(turn) * plane_fs + to_place, to_tp, to_place * n_tp + to_tp

    def peer(step):
        paired = 1 - step // (n - 2)
        step = step + (1 - 2 * lax.rem(step, 2)) * paired * 0
        crossing = 1 - lax.rem(step, 2)
        at = lax.rem(step // 2 + 1 - crossing, n // 2)
        to_fs, to_tp, _ = device(2 * crossing + lax.rem(at, 2), at // 2)
        return to_fs, to_tp, to_fs * n_tp + to_tp

    def cross(at):
        to_fs, to_tp, _ = device(2 + lax.rem(at, 2), at // 2)
        return to_fs, to_tp, to_fs * n_tp + to_tp

    def close(at):
        at = lax.rem(at + 1, n // 2)
        to_fs, to_tp, _ = device(lax.rem(at, 2), at // 2)
        return to_fs, to_tp, to_fs * n_tp + to_tp

    def remote(source, target, send, recv, to):
        return pltpu.make_async_remote_copy(
            src_ref=source,
            dst_ref=target,
            send_sem=send,
            recv_sem=recv,
            device_id=(to[0], to[1]),
            device_id_type=MESH,
        )

    barrier = pltpu.get_barrier_semaphore()

    def greet(step, carry):
        to = peer(step)
        pl.semaphore_signal(barrier, inc=1, device_id=(to[0], to[1]), device_id_type=MESH)
        return carry

    loads = [
        pltpu.make_async_copy(source, target, load_sem.at[i])
        for i, (source, target) in enumerate(
            [
                (gain_far, gain),
                (routes_far, routes_t),
                (weight_far, weight_t),
                (tokens_far, tokens),
                (gate, gate_in),
                (up, up_in),
                (down, down_in),
            ]
        )
    ]
    for load in loads:
        load.start()
    lax.fori_loop(0, n - 1, greet, 0)

    for load in loads[:4]:
        load.wait()
    for i in range(tile_rows // lanes):
        gains[i * lanes : (i + 1) * lanes, :] = jnp.transpose(
            jnp.broadcast_to(gain[i : i + 1, :], (tile_cols, lanes))
        )

    def token_copy(turn, source):
        to = 1 if turn == 3 else turn
        return remote(
            source, arrived.at[turn - 1], token_send.at[turn - 1], token_recv.at[turn - 1], device(to, 0)
        )

    def route_copy(turn):
        return remote(
            routes_t, far_routes.at[turn - 1], route_send.at[turn - 1], route_recv.at[turn - 1], device(turn, 0)
        )

    def weight_copy(turn):
        return remote(
            weight_t, far_weight.at[turn - 1], route_send.at[turn + 2], route_recv.at[turn + 2], device(turn, 0)
        )

    token_copies = [
        token_copy(1, tokens),
        token_copy(2, tokens),
        token_copy(3, arrived.at[1]),
    ]
    route_copies = [copy(turn) for copy in (route_copy, weight_copy) for turn in (1, 2, 3)]

    def first_copy(to):
        return remote(
            in_tiles.at[to[2]],
            in_mats.at[
                :,
                pl.ds(pl.multiple_of(fs * tile_rows, tile_rows), tile_rows),
                pl.ds(pl.multiple_of(tp * tile_cols, tile_cols), tile_cols),
            ],
            first_send,
            first_recv,
            to,
        )

    own_rows = pl.ds(pl.multiple_of(fs * down_rows, down_rows), down_rows)
    own_lanes = pl.ds(pl.multiple_of(tp * lanes, lanes), lanes)

    def near_copy(to):
        return remote(
            out_tiles.at[to[2]], out_mat.at[:, own_rows, own_lanes], near_send, near_recv, to
        )

    def second_copy(c, to):
        return remote(
            out_tiles.at[to[2], c],
            out_mat.at[c, own_rows, own_lanes],
            second_send.at[c],
            second_recv.at[c],
            to,
        )

    def cast_first(step):
        e = peer(step)[2]
        in_tiles[e, 0] = (gate_in[e] * gains[...]).astype(jnp.bfloat16)
        in_tiles[e, 1] = (up_in[e] * gains[...]).astype(jnp.bfloat16)

    def cast_second(step):
        e = peer(step)[2]
        for c in range(chunks):
            out_tiles[e, c] = down_in[e, :, c * lanes : (c + 1) * lanes].astype(jnp.bfloat16)

    def send_first(step, carry):
        cast_first(step + 1)
        first_copy(peer(step)).start()
        return carry

    before = (
        lax.broadcasted_iota(jnp.int32, (tok_rows, tok_rows), 0)
        < lax.broadcasted_iota(jnp.int32, (tok_rows, tok_rows), 1)
    ).astype(jnp.float32).astype(jnp.bfloat16)

    experts = lax.broadcasted_iota(jnp.int32, (plane, tok_rows), 0) + layer * plane
    number = lax.broadcasted_iota(jnp.int32, (plane, capacity, tok_rows), 1).astype(jnp.float32)

    def named_in(paths, shares):
        named = jnp.zeros((plane, tok_rows), jnp.float32)
        scaled = jnp.zeros((plane, tok_rows), jnp.float32)
        for k in range(per_token):
            hit = paths[k : k + 1, :] == experts
            named = named + hit.astype(jnp.float32)
            if shares is not None:
                scaled = scaled + jnp.where(hit, shares[k : k + 1, :], 0.0)
        rank = jnp.dot(named.astype(jnp.bfloat16), before, preferred_element_type=jnp.float32)
        rank = jnp.where(named > 0.5, rank, -1.0)
        return (rank[:, None, :] == number).astype(jnp.float32), scaled

    def normalize(turn, rows_ref):
        values = rows_ref[...].astype(jnp.float32)
        squares = jnp.mean(values * values, axis=1, keepdims=True)
        normed[turn] = (values * lax.rsqrt(squares + norm_epsilon)).astype(jnp.bfloat16)

    def fill_slots(turn, paths):
        select, _ = named_in(paths, None)
        rows = jnp.dot(
            select.reshape(plane * capacity, tok_rows).astype(jnp.bfloat16),
            normed[turn],
            preferred_element_type=jnp.float32,
        )
        slots_out[:, turn] = rows.reshape(plane, capacity, width).astype(jnp.bfloat16)

    def fill_mix(turn, paths, shares):
        select, scaled = named_in(paths, shares)
        picks = jnp.transpose((select * scaled[:, None, :]).reshape(plane * capacity, tok_rows))
        high = picks.astype(jnp.bfloat16)
        mix_high[turn] = high
        mix_low[turn] = (picks - high.astype(jnp.float32)).astype(jnp.bfloat16)

    def slot_copy(turn, to):
        return remote(
            slots_out.at[to[2], turn], slots_in.at[spot, turn], slot_send, slot_recv, to
        )

    def send_slots(turn):
        def send_one(step, carry):
            slot_copy(turn, device(0, step)).start()
            return carry

        lax.fori_loop(1, plane, send_one, 0)
        slots_in[spot, turn] = slots_out[spot, turn]

    def send_some(start, stop):
        lax.fori_loop(start, stop, send_first, 0)

    normalize(0, tokens)
    pl.semaphore_wait(barrier, n - 1)
    for each in route_copies:
        each.start()
    token_copies[1].start()
    token_copies[0].start()
    fill_slots(0, routes_t)
    loads[4].wait()
    loads[5].wait()
    cast_first(0)
    send_some(0, n // 8)
    send_slots(0)
    send_some(n // 8, 3 * n // 8)
    for each in route_copies:
        each.wait_recv()
    token_copies[1].wait_recv()
    token_copies[2].start()
    normalize(2, arrived.at[1])
    fill_slots(2, far_routes.at[1])
    send_some(3 * n // 8, n // 2)
    send_slots(2)
    token_copies[0].wait_recv()
    normalize(1, arrived.at[0])
    fill_slots(1, far_routes.at[0])
    send_some(n // 2, 5 * n // 8)
    send_slots(1)
    token_copies[2].wait_recv()
    normalize(3, arrived.at[2])
    fill_slots(3, far_routes.at[2])
    send_some(5 * n // 8, 6 * n // 8)
    send_slots(3)
    send_some(6 * n // 8, n - 1)

    me = fs * n_tp + tp
    mine_rows = pl.ds(pl.multiple_of(fs * tile_rows, tile_rows), tile_rows)
    mine_cols = pl.ds(pl.multiple_of(tp * tile_cols, tile_cols), tile_cols)
    in_mats[0, mine_rows, mine_cols] = in_tiles[me, 0]
    in_mats[1, mine_rows, mine_cols] = in_tiles[me, 1]

    loads[6].wait()
    cast_second(0)
    cast_second(1)

    def send_second(step, carry):
        cast_second(2 * step + 2)
        cast_second(2 * step + 3)
        second_copy(0, cross(step)).start()
        return carry

    lax.fori_loop(0, n // 2 - 1, send_second, 0)
    second_copy(0, cross(n // 2 - 1)).start()

    def send_near(step, carry):
        near_copy(close(step)).start()
        return carry

    lax.fori_loop(0, n // 2 - 1, send_near, 0)
    out_mat[:, own_rows, own_lanes] = out_tiles[me]

    def send_chunk(c):
        def send_one(step, carry):
            second_copy(c, cross(step)).start()
            return carry

        lax.fori_loop(0, n // 2, send_one, 0)

    send_chunk(1)
    fill_mix(0, routes_t, weight_t)
    for turn in range(1, planes):
        fill_mix(turn, far_routes.at[turn - 1], far_weight.at[turn - 1])

    near = device(1, 0)

    def take(size_ref, send, recv):
        return remote(size_ref, size_ref, send, recv, near)

    slots_all = take(slots_in.at[pl.ds(0, plane - 1)], slot_send, slot_recv)
    first_all = take(in_tiles.at[pl.ds(0, n - 1)], first_send, first_recv)
    near_all = take(out_tiles.at[pl.ds(0, n // 2 - 1)], near_send, near_recv)

    def second_all(c):
        return take(out_tiles.at[pl.ds(0, n // 2), c], second_send.at[c], second_recv.at[c])

    def back_all(j):
        return take(rows_in.at[j, pl.ds(0, plane - 1)], back_send.at[j], back_recv.at[j])

    slots_all.wait_recv()
    first_all.wait_recv()

    group = active.shape[1]
    held = group // (planes * capacity)

    def activate(g, carry):
        inputs = slots_in[pl.ds(g * held, held)].astype(jnp.float32)
        inputs = inputs.reshape(group, width).astype(jnp.bfloat16)
        gate_pre = jnp.dot(inputs, in_mats[0], preferred_element_type=jnp.float32)
        up_pre = jnp.dot(inputs, in_mats[1], preferred_element_type=jnp.float32)
        gate_part = jnp.minimum(gate_pre, clamp_limit)
        linear_part = jnp.clip(up_pre, -clamp_limit, clamp_limit)
        active[g] = (
            gate_part * jax.nn.sigmoid(sigmoid_slope * gate_part) * (linear_part + 1.0)
        ).astype(jnp.bfloat16)
        return carry

    lax.fori_loop(0, active.shape[0], activate, 0)
    near_all.wait_recv()

    pieces, piece = rows_out.shape[0], rows_out.shape[-1]
    split = pieces // chunks

    def back_copy(j, shift):
        to = device(0, shift)
        return remote(
            rows_out.at[j, to[2]], rows_in.at[j, spot], back_send.at[j], back_recv.at[j], to
        )

    def side_copy(j):
        return remote(side_out.at[j], side_in.at[j], side_send.at[j], side_recv.at[j], device(1, 0))

    def part_copy(j):
        return remote(part_out.at[j], part_in.at[j], part_send.at[j], part_recv.at[j], device(2, 0))

    def project(c):
        second_all(c).wait_recv()
        for i in range(split):
            j = c * split + i

            def project_group(g, carry):
                rows = jnp.dot(
                    active[g],
                    out_mat[c, :, i * piece : (i + 1) * piece],
                    preferred_element_type=jnp.float32,
                )
                rows_out[j, pl.ds(g * held, held)] = rows.reshape(
                    held, planes, capacity, piece
                ).astype(jnp.bfloat16)
                return carry

            lax.fori_loop(0, active.shape[0], project_group, 0)

            def send_back(step, carry):
                back_copy(j, step).start()
                return carry

            lax.fori_loop(1, plane, send_back, 0)
            rows_in[j, spot] = rows_out[j, spot]

    span = plane * capacity

    def combine(j, turn):
        rows = rows_in[j, :, turn].astype(jnp.float32).reshape(span, piece).astype(jnp.bfloat16)
        total = jnp.dot(mix_high[turn], rows, preferred_element_type=jnp.float32)
        return total + jnp.dot(mix_low[turn], rows, preferred_element_type=jnp.float32)

    def give_side(j):
        back_all(j).wait_recv()
        for q in range(2):
            side_out[j, q] = combine(j, 2 * q + 1).astype(jnp.bfloat16)
        for q in range(1, -1, -1):
            totals[j, q] = combine(j, 2 * q)
            if q == 1:
                side_copy(j).start()

    def give_part(j):
        side_copy(j).wait_recv()
        part_out[j] = (totals[j, 1] + side_in[j, 1].astype(jnp.float32)).astype(jnp.bfloat16)
        totals[j, 0] = totals[j, 0] + side_in[j, 0].astype(jnp.float32)
        part_copy(j).start()

    def finish(j):
        part_copy(j).wait_recv()
        total = (totals[j, 0] + part_in[j].astype(jnp.float32)).astype(jnp.bfloat16)
        for k in range(piece // lanes):
            slab = j % split * (piece // lanes) + k
            start = slab * down_cols + j // split * lanes
            mixed[:, start : start + lanes] = total[:, k * lanes : (k + 1) * lanes]

    def run(stage, c):
        for i in range(split):
            stage(c * split + i)

    for c in range(chunks):
        project(c)
        if c > 0:
            run(give_side, c - 1)
        if c + 2 < chunks:
            send_chunk(c + 2)
        if c > 1:
            run(give_part, c - 2)
    for i in range(split):
        give_side((chunks - 1) * split + i)
        if i == 0:
            run(give_part, chunks - 2)
    run(give_part, chunks - 1)
    for j in range(pieces):
        finish(j)

    first_all.wait_send()
    near_all.wait_send()
    slots_all.wait_send()
    for c in range(chunks):
        second_all(c).wait_send()
    for j in range(pieces):
        back_all(j).wait_send()
        side_copy(j).wait_send()
        part_copy(j).wait_send()
    for each in token_copies + route_copies:
        each.wait_send()


def keep_kernel(in_mats, out_mat, rows, gate_out, up_out, down_out, mixed, sem):
    chunks, _, block = out_mat.shape
    n_tp = block // 128
    lanes = block // n_tp
    down_cols = chunks * lanes
    copies = [
        (in_mats.at[0], gate_out.at[0]),
        (in_mats.at[1], up_out.at[0]),
        (rows, mixed),
    ]
    for c in range(chunks):
        for k in range(n_tp):
            start = k * down_cols + c * lanes
            copies.append(
                (
                    out_mat.at[c, :, k * lanes : (k + 1) * lanes],
                    down_out.at[0, :, start : start + lanes],
                )
            )
    copies = [
        pltpu.make_async_copy(source, target, sem.at[i])
        for i, (source, target) in enumerate(copies)
    ]
    for copy in copies:
        copy.start()
    for copy in copies:
        copy.wait()


def direct_shards(
    tokens, routes, route_weight, norm_gain, gate_weight, up_weight, down_weight
):
    n_fs, n_tp = lax.axis_size("fs"), lax.axis_size("tp")
    n = n_fs * n_tp
    tok_rows, width = tokens.shape
    tile_rows, tile_cols = gate_weight.shape[1:]
    down_rows, down_cols = down_weight.shape[1:]
    hidden = n_tp * tile_cols
    lanes = 128
    chunks = down_cols // lanes
    block = n_tp * lanes
    plane = n // 4
    pieces, piece = chunks * 2, block // 2
    per_token = routes.shape[1]
    capacity = max(2, 3 * tok_rows * per_token // (2 * n))
    bf16, f32 = jnp.bfloat16, jnp.float32
    whole = pl.BlockSpec(memory_space=pltpu.VMEM)
    apart = pl.BlockSpec(memory_space=pltpu.HBM)
    dma = pltpu.SemaphoreType.DMA
    groups = 4
    in_mats, out_mat, rows = pl.pallas_call(
        functools.partial(exchange_kernel, (n_fs, n_tp, capacity)),
        out_shape=(
            pltpu.VMEM((2, width, hidden), bf16),
            pltpu.VMEM((chunks, hidden, block), bf16),
            pltpu.VMEM((tok_rows, width), bf16),
        ),
        in_specs=[apart] * 7,
        out_specs=(whole, whole, whole),
        scratch_shapes=[
            pltpu.VMEM((tok_rows, width), tokens.dtype),
            pltpu.VMEM((per_token, tok_rows), routes.dtype),
            pltpu.VMEM((per_token, tok_rows), f32),
            pltpu.VMEM((tile_rows // lanes, lanes), f32),
            pltpu.VMEM((n, tile_rows, tile_cols), f32),
            pltpu.VMEM((n, tile_rows, tile_cols), f32),
            pltpu.VMEM((n, down_rows, down_cols), f32),
            pltpu.VMEM((tile_rows, tile_cols), f32),
            pltpu.VMEM((n, 2, tile_rows, tile_cols), bf16),
            pltpu.VMEM((n, chunks, down_rows, lanes), bf16),
            pltpu.VMEM((3, tok_rows, width), bf16),
            pltpu.VMEM((4, tok_rows, width), bf16),
            pltpu.VMEM((plane, 4, capacity, width), bf16),
            pltpu.VMEM((plane, 4, capacity, width), bf16),
            pltpu.VMEM((groups, n * capacity // groups, hidden), bf16),
            pltpu.VMEM((3, per_token, tok_rows), routes.dtype),
            pltpu.VMEM((3, per_token, tok_rows), f32),
            pltpu.VMEM((4, tok_rows, plane * capacity), bf16),
            pltpu.VMEM((4, tok_rows, plane * capacity), bf16),
            pltpu.VMEM((pieces, plane, 4, capacity, piece), bf16),
            pltpu.VMEM((pieces, plane, 4, capacity, piece), bf16),
            pltpu.VMEM((pieces, 2, tok_rows, piece), bf16),
            pltpu.VMEM((pieces, 2, tok_rows, piece), bf16),
            pltpu.VMEM((pieces, 2, tok_rows, piece), f32),
            pltpu.VMEM((pieces, tok_rows, piece), bf16),
            pltpu.VMEM((pieces, tok_rows, piece), bf16),
            dma((7,)),
            dma((3,)),
            dma((3,)),
            dma((6,)),
            dma((6,)),
            dma,
            dma,
            dma,
            dma,
            dma,
            dma,
        ]
        + [dma((chunks,))] * 2
        + [dma((pieces,))] * 6,
        compiler_params=pltpu.CompilerParams(
            collective_id=0, has_side_effects=True, vmem_limit_bytes=52 * 1024 * 1024
        ),
    )(
        tokens,
        routes.T,
        route_weight.T,
        norm_gain.reshape(tile_rows // lanes, lanes),
        gate_weight,
        up_weight,
        down_weight,
    )
    return pl.pallas_call(
        keep_kernel,
        out_shape=(
            jax.ShapeDtypeStruct((1, width, hidden), bf16),
            jax.ShapeDtypeStruct((1, width, hidden), bf16),
            jax.ShapeDtypeStruct((1, hidden, width), bf16),
            jax.ShapeDtypeStruct((tok_rows, width), bf16),
        ),
        in_specs=[whole] * 3,
        out_specs=(apart,) * 4,
        scratch_shapes=[dma((3 + chunks * n_tp,))],
        compiler_params=pltpu.CompilerParams(vmem_limit_bytes=8 * 1024 * 1024),
    )(in_mats, out_mat, rows)


def aligned(mesh, tokens, routes, gate_weight, down_weight):
    n_fs, n_tp = mesh.shape["fs"], mesh.shape["tp"]
    n = n_fs * n_tp
    tok_rows = tokens.shape[0] // n
    capacity = max(2, 3 * tok_rows * routes.shape[1] // (2 * n))
    return (
        gate_weight.shape[0] == n
        and n_fs % 4 == 0
        and n % 32 == 0
        and capacity % 8 == 0
        and tok_rows % 128 == 0
        and tokens.shape[1] % 512 == 0
        and gate_weight.shape[1] // n_fs % 128 == 0
        and gate_weight.shape[2] // n_tp % 128 == 0
        and down_weight.shape[1] // n_fs % 16 == 0
        and down_weight.shape[2] // n_tp % 128 == 0
    )


def solution(mesh):
    placed = (
        P(("fs", "tp"), None),
        P(("fs", "tp"), None),
        P(("fs", "tp"), None),
        P("fs"),
        P(None, "fs", "tp"),
        P(None, "fs", "tp"),
        P(None, "fs", "tp"),
    )

    def run(tokens, routes, route_weight, norm_gain, gate_weight, up_weight, down_weight):
        direct = aligned(mesh, tokens, routes, gate_weight, down_weight)
        return jax.shard_map(
            direct_shards if direct else shards,
            mesh=mesh,
            in_specs=placed,
            out_specs=(
                P(("fs", "tp"), None, None),
                P(("fs", "tp"), None, None),
                P(("fs", "tp"), None, None),
                P(("fs", "tp"), None),
            ),
            check_vma=False,
        )(tokens, routes, route_weight, norm_gain, gate_weight, up_weight, down_weight)

    return run
```

```python
import functools

import jax
import jax.numpy as jnp
from jax import lax
from jax.experimental import pallas as pl
from jax.experimental.pallas import tpu as pltpu
from jax.sharding import PartitionSpec as P

norm_epsilon = 1e-06
clamp_limit = 7.0
sigmoid_slope = 1.702
MESH = pl.DeviceIdType.MESH


def feed(inputs, gate_mat, up_mat, down_mat):
    gate_pre = jnp.dot(inputs, gate_mat, preferred_element_type=jnp.float32)
    up_pre = jnp.dot(inputs, up_mat, preferred_element_type=jnp.float32)
    gate_part = jnp.minimum(gate_pre, clamp_limit)
    linear_part = jnp.clip(up_pre, -clamp_limit, clamp_limit)
    activation = (
        gate_part * jax.nn.sigmoid(sigmoid_slope * gate_part) * (linear_part + 1.0)
    ).astype(jnp.bfloat16)
    return jnp.dot(activation, down_mat, preferred_element_type=jnp.float32).astype(jnp.bfloat16)


def assemble(received, rows_groups, column_groups):
    tile_rows = received.shape[2]
    tile_columns = received.shape[3]
    sources = received.reshape(rows_groups, column_groups, tile_rows, tile_columns)
    return sources.transpose(0, 2, 1, 3).reshape(
        1, rows_groups * tile_rows, column_groups * tile_columns
    )


def shards(tokens, routes, route_weight, norm_gain, gate_weight, up_weight, down_weight):
    gain_column = norm_gain[None, :, None]
    gate_tiles = (gate_weight * gain_column).astype(jnp.bfloat16)
    up_tiles = (up_weight * gain_column).astype(jnp.bfloat16)
    down_tiles = down_weight.astype(jnp.bfloat16)
    rows_groups = lax.axis_size("fs")
    column_groups = lax.axis_size("tp")
    arrived = (
        lax.all_to_all(gate_tiles[:, None], ("fs", "tp"), split_axis=0, concat_axis=1, tiled=True),
        lax.all_to_all(up_tiles[:, None], ("fs", "tp"), split_axis=0, concat_axis=1, tiled=True),
        lax.all_to_all(down_tiles[:, None], ("fs", "tp"), split_axis=0, concat_axis=1, tiled=True),
    )
    gate_new = assemble(arrived[0], rows_groups, column_groups)
    up_new = assemble(arrived[1], rows_groups, column_groups)
    down_new = assemble(arrived[2], rows_groups, column_groups)
    experts = rows_groups * column_groups
    tok_rows, model_width = tokens.shape
    per_token = routes.shape[1]
    capacity = max(2, 3 * tok_rows * per_token // (2 * experts))
    values = tokens.astype(jnp.float32)
    squares = jnp.mean(values * values, axis=1, keepdims=True)
    normed = (values * lax.rsqrt(squares + norm_epsilon)).astype(jnp.bfloat16)
    flat_routes = routes.reshape(-1)
    onehot = (flat_routes[:, None] == jnp.arange(experts, dtype=jnp.int32)[None, :]).astype(
        jnp.int32
    )
    earlier = jnp.cumsum(onehot, axis=0) - onehot
    rank = jnp.sum(earlier * onehot, axis=1)
    slot_index = flat_routes * capacity + rank
    slot_numbers = jnp.arange(experts * capacity, dtype=jnp.int32)
    select = jnp.any(
        slot_index.reshape(tok_rows, per_token)[None, :, :] == slot_numbers[:, None, None], axis=2
    )
    buffer = jnp.dot(
        select.astype(jnp.bfloat16), normed, preferred_element_type=jnp.float32
    ).astype(jnp.bfloat16)
    buffer = buffer.reshape(experts, 1, capacity, model_width)
    slot_rows = lax.all_to_all(buffer, ("fs", "tp"), split_axis=0, concat_axis=1, tiled=True)
    sources = slot_rows.shape[1]
    count = slot_rows.shape[2]
    expert_out = feed(slot_rows.reshape(-1, model_width), gate_new[0], up_new[0], down_new[0])
    expert_out = expert_out.reshape(1, sources, count, model_width)
    returned = lax.all_to_all(expert_out, ("fs", "tp"), split_axis=1, concat_axis=0, tiled=True)
    returned = returned.reshape(experts * capacity, model_width)
    picked = returned[slot_index].reshape(tok_rows, per_token, model_width)
    mixed = jnp.sum(picked.astype(jnp.float32) * route_weight[:, :, None], axis=1).astype(
        jnp.bfloat16
    )
    return (gate_new, up_new, down_new, mixed)


def exchange_kernel(
    sizes, tokens_far, routes_far, weight_far, gain_far, gate, up, down,
    in_mats, out_mat, mixed,
    tokens, routes_t, weight_t, gain, gate_in, up_in, down_in, gains, in_tiles, out_tiles,
    arrived, normed, slots_out, slots_in, active, far_routes, far_weight,
    mix_high, mix_low, rows_out, rows_in, side_out, side_in, totals, part_out, part_in,
    load_sem, token_send, token_recv, route_send, route_recv,
    first_send, first_recv, near_send, near_recv, slot_send, slot_recv,
    second_send, second_recv, back_send, back_recv, side_send, side_recv, part_send, part_recv, ready,
):
    n_fs, n_tp, capacity = sizes
    n = n_fs * n_tp
    fs, tp = lax.axis_index("fs"), lax.axis_index("tp")
    tok_rows, width = tokens.shape
    tile_rows, tile_cols = gate_in.shape[1:]
    chunks, down_rows, lanes = out_tiles.shape[1:]
    down_cols = chunks * lanes
    block = n_tp * lanes
    per_token = routes_t.shape[0]

    planes = 4
    plane_fs = n_fs // planes
    plane = n // planes
    layer, place = fs // plane_fs, lax.rem(fs, plane_fs)
    spot = place * n_tp + tp

    def flip(turn):
        low = lax.rem(layer + turn, 2)
        high = lax.rem(layer // 2 + turn // 2, 2)
        return 2 * high + low

    def device(turn, shift):
        to_place = lax.rem(place + shift // n_tp, plane_fs)
        to_tp = lax.rem(tp + lax.rem(shift, n_tp), n_tp)
        return flip(turn) * plane_fs + to_place, to_tp, to_place * n_tp + to_tp

    def peer(step):
        paired = 1 - step // (n - 2)
        step = step + (1 - 2 * lax.rem(step, 2)) * paired * 0
        crossing = 1 - lax.rem(step, 2)
        at = lax.rem(step // 2 + 1 - crossing, n // 2)
        to_fs, to_tp, _ = device(2 * crossing + lax.rem(at, 2), at // 2)
        return to_fs, to_tp, to_fs * n_tp + to_tp

    def cross(at):
        to_fs, to_tp, _ = device(2 + lax.rem(at, 2), at // 2)
        return to_fs, to_tp, to_fs * n_tp + to_tp

    def close(at):
        at = lax.rem(at + 1, n // 2)
        to_fs, to_tp, _ = device(lax.rem(at, 2), at // 2)
        return to_fs, to_tp, to_fs * n_tp + to_tp

    def remote(source, target, send, recv, to):
        return pltpu.make_async_remote_copy(
            src_ref=source,
            dst_ref=target,
            send_sem=send,
            recv_sem=recv,
            device_id=(to[0], to[1]),
            device_id_type=MESH,
        )

    barrier = pltpu.get_barrier_semaphore()

    across = [device(turn, 0) for turn in range(1, planes)]
    aside = [device(0, shift) for shift in range(1, n_tp)]
    along = [device(0, shift * n_tp) for shift in range(1, plane_fs)]

    def greet(semaphore, group):
        for to in group:
            pl.semaphore_signal(semaphore, inc=1, device_id=(to[0], to[1]), device_id_type=MESH)

    loads = [
        pltpu.make_async_copy(source, target, load_sem.at[i])
        for i, (source, target) in enumerate(
            [
                (gain_far, gain),
                (routes_far, routes_t),
                (weight_far, weight_t),
                (tokens_far, tokens),
                (gate, gate_in),
                (up, up_in),
                (down, down_in),
            ]
        )
    ]
    for load in loads:
        load.start()
    greet(barrier, across + along + aside)

    for load in loads[:4]:
        load.wait()
    for i in range(tile_rows // lanes):
        gains[i * lanes : (i + 1) * lanes, :] = jnp.transpose(
            jnp.broadcast_to(gain[i : i + 1, :], (tile_cols, lanes))
        )

    def token_copy(turn, source):
        to = 1 if turn == 3 else turn
        return remote(
            source, arrived.at[turn - 1], token_send.at[turn - 1], token_recv.at[turn - 1], device(to, 0)
        )

    def route_copy(turn):
        return remote(
            routes_t, far_routes.at[turn - 1], route_send.at[turn - 1], route_recv.at[turn - 1], device(turn, 0)
        )

    def weight_copy(turn):
        return remote(
            weight_t, far_weight.at[turn - 1], route_send.at[turn + 2], route_recv.at[turn + 2], device(turn, 0)
        )

    token_copies = [
        token_copy(1, tokens),
        token_copy(2, tokens),
        token_copy(3, arrived.at[1]),
    ]
    route_copies = [copy(turn) for copy in (route_copy, weight_copy) for turn in (1, 2, 3)]

    def first_copy(to):
        return remote(
            in_tiles.at[to[2]],
            in_mats.at[
                :,
                pl.ds(pl.multiple_of(fs * tile_rows, tile_rows), tile_rows),
                pl.ds(pl.multiple_of(tp * tile_cols, tile_cols), tile_cols),
            ],
            first_send,
            first_recv,
            to,
        )

    own_rows = pl.ds(pl.multiple_of(fs * down_rows, down_rows), down_rows)
    own_lanes = pl.ds(pl.multiple_of(tp * lanes, lanes), lanes)

    def near_copy(to):
        return remote(
            out_tiles.at[to[2]], out_mat.at[:, own_rows, own_lanes], near_send, near_recv, to
        )

    def second_copy(c, to):
        return remote(
            out_tiles.at[to[2], c],
            out_mat.at[c, own_rows, own_lanes],
            second_send.at[c],
            second_recv.at[c],
            to,
        )

    def cast_first(step):
        e = peer(step)[2]
        in_tiles[e, 0] = (gate_in[e] * gains[...]).astype(jnp.bfloat16)
        in_tiles[e, 1] = (up_in[e] * gains[...]).astype(jnp.bfloat16)

    def cast_second(step):
        e = peer(step)[2]
        for c in range(chunks):
            out_tiles[e, c] = down_in[e, :, c * lanes : (c + 1) * lanes].astype(jnp.bfloat16)

    def send_first(step, carry):
        cast_first(step + 1)
        first_copy(peer(step)).start()
        return carry

    before = (
        lax.broadcasted_iota(jnp.int32, (tok_rows, tok_rows), 0)
        < lax.broadcasted_iota(jnp.int32, (tok_rows, tok_rows), 1)
    ).astype(jnp.float32).astype(jnp.bfloat16)

    experts = lax.broadcasted_iota(jnp.int32, (plane, tok_rows), 0) + layer * plane
    number = lax.broadcasted_iota(jnp.int32, (plane, capacity, tok_rows), 1).astype(jnp.float32)

    def named_in(paths, shares):
        named = jnp.zeros((plane, tok_rows), jnp.float32)
        scaled = jnp.zeros((plane, tok_rows), jnp.float32)
        for k in range(per_token):
            hit = paths[k : k + 1, :] == experts
            named = named + hit.astype(jnp.float32)
            if shares is not None:
                scaled = scaled + jnp.where(hit, shares[k : k + 1, :], 0.0)
        rank = jnp.dot(named.astype(jnp.bfloat16), before, preferred_element_type=jnp.float32)
        rank = jnp.where(named > 0.5, rank, -1.0)
        return (rank[:, None, :] == number).astype(jnp.float32), scaled

    def normalize(turn, rows_ref):
        values = rows_ref[...].astype(jnp.float32)
        squares = jnp.mean(values * values, axis=1, keepdims=True)
        normed[turn] = (values * lax.rsqrt(squares + norm_epsilon)).astype(jnp.bfloat16)

    def fill_slots(turn, paths):
        select, _ = named_in(paths, None)
        rows = jnp.dot(
            select.reshape(plane * capacity, tok_rows).astype(jnp.bfloat16),
            normed[turn],
            preferred_element_type=jnp.float32,
        )
        slots_out[:, turn] = rows.reshape(plane, capacity, width).astype(jnp.bfloat16)

    def fill_mix(turn, paths, shares):
        select, scaled = named_in(paths, shares)
        picks = jnp.transpose((select * scaled[:, None, :]).reshape(plane * capacity, tok_rows))
        high = picks.astype(jnp.bfloat16)
        mix_high[turn] = high
        mix_low[turn] = (picks - high.astype(jnp.float32)).astype(jnp.bfloat16)

    def slot_copy(turn, to):
        return remote(
            slots_out.at[to[2], turn], slots_in.at[spot, turn], slot_send, slot_recv, to
        )

    def send_slots(turn):
        def send_one(step, carry):
            slot_copy(turn, device(0, step)).start()
            return carry

        lax.fori_loop(1, plane, send_one, 0)
        slots_in[spot, turn] = slots_out[spot, turn]

    def send_some(start, stop):
        lax.fori_loop(start, stop, send_first, 0)

    normalize(0, tokens)
    pl.semaphore_wait(barrier, len(across + along + aside))
    greet(ready.at[0], aside)
    for each in route_copies:
        each.start()
    token_copies[1].start()
    token_copies[0].start()
    pl.semaphore_wait(ready.at[0], len(aside))
    greet(ready.at[1], along)
    fill_slots(0, routes_t)
    loads[4].wait()
    loads[5].wait()
    cast_first(0)
    pl.semaphore_wait(ready.at[1], len(along))
    send_some(0, n // 8)
    send_slots(0)
    send_some(n // 8, 3 * n // 8)
    for each in route_copies:
        each.wait_recv()
    token_copies[1].wait_recv()
    token_copies[2].start()
    normalize(2, arrived.at[1])
    fill_slots(2, far_routes.at[1])
    send_some(3 * n // 8, n // 2)
    send_slots(2)
    token_copies[0].wait_recv()
    normalize(1, arrived.at[0])
    fill_slots(1, far_routes.at[0])
    send_some(n // 2, 5 * n // 8)
    send_slots(1)
    token_copies[2].wait_recv()
    normalize(3, arrived.at[2])
    fill_slots(3, far_routes.at[2])
    send_some(5 * n // 8, 6 * n // 8)
    send_slots(3)
    send_some(6 * n // 8, n - 1)

    me = fs * n_tp + tp
    mine_rows = pl.ds(pl.multiple_of(fs * tile_rows, tile_rows), tile_rows)
    mine_cols = pl.ds(pl.multiple_of(tp * tile_cols, tile_cols), tile_cols)
    in_mats[0, mine_rows, mine_cols] = in_tiles[me, 0]
    in_mats[1, mine_rows, mine_cols] = in_tiles[me, 1]

    loads[6].wait()
    cast_second(0)
    cast_second(1)

    def send_second(step, carry):
        cast_second(2 * step + 2)
        cast_second(2 * step + 3)
        second_copy(0, cross(step)).start()
        return carry

    lax.fori_loop(0, n // 2 - 1, send_second, 0)
    second_copy(0, cross(n // 2 - 1)).start()

    def send_near(step, carry):
        near_copy(close(step)).start()
        return carry

    lax.fori_loop(0, n // 2 - 1, send_near, 0)
    out_mat[:, own_rows, own_lanes] = out_tiles[me]

    def send_chunk(c):
        def send_one(step, carry):
            second_copy(c, cross(step)).start()
            return carry

        lax.fori_loop(0, n // 2, send_one, 0)

    send_chunk(1)
    fill_mix(0, routes_t, weight_t)
    for turn in range(1, planes):
        fill_mix(turn, far_routes.at[turn - 1], far_weight.at[turn - 1])

    near = device(1, 0)

    def take(size_ref, send, recv):
        return remote(size_ref, size_ref, send, recv, near)

    slots_all = take(slots_in.at[pl.ds(0, plane - 1)], slot_send, slot_recv)
    first_all = take(in_tiles.at[pl.ds(0, n - 1)], first_send, first_recv)
    near_all = take(out_tiles.at[pl.ds(0, n // 2 - 1)], near_send, near_recv)

    def second_all(c):
        return take(out_tiles.at[pl.ds(0, n // 2), c], second_send.at[c], second_recv.at[c])

    def back_all(j):
        return take(rows_in.at[j, pl.ds(0, plane - 1)], back_send.at[j], back_recv.at[j])

    slots_all.wait_recv()
    first_all.wait_recv()

    group = active.shape[1]
    held = group // (planes * capacity)

    def activate(g, carry):
        inputs = slots_in[pl.ds(g * held, held)].astype(jnp.float32)
        inputs = inputs.reshape(group, width).astype(jnp.bfloat16)
        gate_pre = jnp.dot(inputs, in_mats[0], preferred_element_type=jnp.float32)
        up_pre = jnp.dot(inputs, in_mats[1], preferred_element_type=jnp.float32)
        gate_part = jnp.minimum(gate_pre, clamp_limit)
        linear_part = jnp.clip(up_pre, -clamp_limit, clamp_limit)
        active[g] = (
            gate_part * jax.nn.sigmoid(sigmoid_slope * gate_part) * (linear_part + 1.0)
        ).astype(jnp.bfloat16)
        return carry

    lax.fori_loop(0, active.shape[0], activate, 0)
    near_all.wait_recv()

    pieces, piece = rows_out.shape[0], rows_out.shape[-1]
    split = pieces // chunks

    def back_copy(j, shift):
        to = device(0, shift)
        return remote(
            rows_out.at[j, to[2]], rows_in.at[j, spot], back_send.at[j], back_recv.at[j], to
        )

    def side_copy(j):
        return remote(side_out.at[j], side_in.at[j], side_send.at[j], side_recv.at[j], device(1, 0))

    def part_copy(j):
        return remote(part_out.at[j], part_in.at[j], part_send.at[j], part_recv.at[j], device(2, 0))

    def project(c):
        second_all(c).wait_recv()
        for i in range(split):
            j = c * split + i

            def project_group(g, carry):
                rows = jnp.dot(
                    active[g],
                    out_mat[c, :, i * piece : (i + 1) * piece],
                    preferred_element_type=jnp.float32,
                )
                rows_out[j, pl.ds(g * held, held)] = rows.reshape(
                    held, planes, capacity, piece
                ).astype(jnp.bfloat16)
                return carry

            lax.fori_loop(0, active.shape[0], project_group, 0)

            def send_back(step, carry):
                back_copy(j, step).start()
                return carry

            lax.fori_loop(1, plane, send_back, 0)
            rows_in[j, spot] = rows_out[j, spot]

    span = plane * capacity

    def combine(j, turn):
        rows = rows_in[j, :, turn].astype(jnp.float32).reshape(span, piece).astype(jnp.bfloat16)
        total = jnp.dot(mix_high[turn], rows, preferred_element_type=jnp.float32)
        return total + jnp.dot(mix_low[turn], rows, preferred_element_type=jnp.float32)

    def give_side(j):
        back_all(j).wait_recv()
        for q in range(2):
            side_out[j, q] = combine(j, 2 * q + 1).astype(jnp.bfloat16)
        for q in range(1, -1, -1):
            totals[j, q] = combine(j, 2 * q)
            if q == 1:
                side_copy(j).start()

    def give_part(j):
        side_copy(j).wait_recv()
        part_out[j] = (totals[j, 1] + side_in[j, 1].astype(jnp.float32)).astype(jnp.bfloat16)
        totals[j, 0] = totals[j, 0] + side_in[j, 0].astype(jnp.float32)
        part_copy(j).start()

    def finish(j):
        part_copy(j).wait_recv()
        total = (totals[j, 0] + part_in[j].astype(jnp.float32)).astype(jnp.bfloat16)
        for k in range(piece // lanes):
            slab = j % split * (piece // lanes) + k
            start = slab * down_cols + j // split * lanes
            mixed[:, start : start + lanes] = total[:, k * lanes : (k + 1) * lanes]

    def run(stage, c):
        for i in range(split):
            stage(c * split + i)

    for c in range(chunks):
        project(c)
        if c > 0:
            run(give_side, c - 1)
        if c + 2 < chunks:
            send_chunk(c + 2)
        if c > 1:
            run(give_part, c - 2)
    for i in range(split):
        give_side((chunks - 1) * split + i)
        if i == 0:
            run(give_part, chunks - 2)
    run(give_part, chunks - 1)
    for j in range(pieces):
        finish(j)

    first_all.wait_send()
    near_all.wait_send()
    slots_all.wait_send()
    for c in range(chunks):
        second_all(c).wait_send()
    for j in range(pieces):
        back_all(j).wait_send()
        side_copy(j).wait_send()
        part_copy(j).wait_send()
    for each in token_copies + route_copies:
        each.wait_send()


def keep_kernel(in_mats, out_mat, rows, gate_out, up_out, down_out, mixed, sem):
    chunks, _, block = out_mat.shape
    n_tp = block // 128
    lanes = block // n_tp
    down_cols = chunks * lanes
    copies = [
        (in_mats.at[0], gate_out.at[0]),
        (in_mats.at[1], up_out.at[0]),
        (rows, mixed),
    ]
    for c in range(chunks):
        for k in range(n_tp):
            start = k * down_cols + c * lanes
            copies.append(
                (
                    out_mat.at[c, :, k * lanes : (k + 1) * lanes],
                    down_out.at[0, :, start : start + lanes],
                )
            )
    copies = [
        pltpu.make_async_copy(source, target, sem.at[i])
        for i, (source, target) in enumerate(copies)
    ]
    for copy in copies:
        copy.start()
    for copy in copies:
        copy.wait()


def direct_shards(
    tokens, routes, route_weight, norm_gain, gate_weight, up_weight, down_weight
):
    n_fs, n_tp = lax.axis_size("fs"), lax.axis_size("tp")
    n = n_fs * n_tp
    tok_rows, width = tokens.shape
    tile_rows, tile_cols = gate_weight.shape[1:]
    down_rows, down_cols = down_weight.shape[1:]
    hidden = n_tp * tile_cols
    lanes = 128
    chunks = down_cols // lanes
    block = n_tp * lanes
    plane = n // 4
    pieces, piece = chunks * 2, block // 2
    per_token = routes.shape[1]
    capacity = max(2, 3 * tok_rows * per_token // (2 * n))
    bf16, f32 = jnp.bfloat16, jnp.float32
    whole = pl.BlockSpec(memory_space=pltpu.VMEM)
    apart = pl.BlockSpec(memory_space=pltpu.HBM)
    dma = pltpu.SemaphoreType.DMA
    groups = 4
    in_mats, out_mat, rows = pl.pallas_call(
        functools.partial(exchange_kernel, (n_fs, n_tp, capacity)),
        out_shape=(
            pltpu.VMEM((2, width, hidden), bf16),
            pltpu.VMEM((chunks, hidden, block), bf16),
            pltpu.VMEM((tok_rows, width), bf16),
        ),
        in_specs=[apart] * 7,
        out_specs=(whole, whole, whole),
        scratch_shapes=[
            pltpu.VMEM((tok_rows, width), tokens.dtype),
            pltpu.VMEM((per_token, tok_rows), routes.dtype),
            pltpu.VMEM((per_token, tok_rows), f32),
            pltpu.VMEM((tile_rows // lanes, lanes), f32),
            pltpu.VMEM((n, tile_rows, tile_cols), f32),
            pltpu.VMEM((n, tile_rows, tile_cols), f32),
            pltpu.VMEM((n, down_rows, down_cols), f32),
            pltpu.VMEM((tile_rows, tile_cols), f32),
            pltpu.VMEM((n, 2, tile_rows, tile_cols), bf16),
            pltpu.VMEM((n, chunks, down_rows, lanes), bf16),
            pltpu.VMEM((3, tok_rows, width), bf16),
            pltpu.VMEM((4, tok_rows, width), bf16),
            pltpu.VMEM((plane, 4, capacity, width), bf16),
            pltpu.VMEM((plane, 4, capacity, width), bf16),
            pltpu.VMEM((groups, n * capacity // groups, hidden), bf16),
            pltpu.VMEM((3, per_token, tok_rows), routes.dtype),
            pltpu.VMEM((3, per_token, tok_rows), f32),
            pltpu.VMEM((4, tok_rows, plane * capacity), bf16),
            pltpu.VMEM((4, tok_rows, plane * capacity), bf16),
            pltpu.VMEM((pieces, plane, 4, capacity, piece), bf16),
            pltpu.VMEM((pieces, plane, 4, capacity, piece), bf16),
            pltpu.VMEM((pieces, 2, tok_rows, piece), bf16),
            pltpu.VMEM((pieces, 2, tok_rows, piece), bf16),
            pltpu.VMEM((pieces, 2, tok_rows, piece), f32),
            pltpu.VMEM((pieces, tok_rows, piece), bf16),
            pltpu.VMEM((pieces, tok_rows, piece), bf16),
            dma((7,)),
            dma((3,)),
            dma((3,)),
            dma((6,)),
            dma((6,)),
            dma,
            dma,
            dma,
            dma,
            dma,
            dma,
        ]
        + [dma((chunks,))] * 2
        + [dma((pieces,))] * 6
        + [pltpu.SemaphoreType.REGULAR((2,))],
        compiler_params=pltpu.CompilerParams(
            collective_id=0, has_side_effects=True, vmem_limit_bytes=52 * 1024 * 1024
        ),
    )(
        tokens,
        routes.T,
        route_weight.T,
        norm_gain.reshape(tile_rows // lanes, lanes),
        gate_weight,
        up_weight,
        down_weight,
    )
    return pl.pallas_call(
        keep_kernel,
        out_shape=(
            jax.ShapeDtypeStruct((1, width, hidden), bf16),
            jax.ShapeDtypeStruct((1, width, hidden), bf16),
            jax.ShapeDtypeStruct((1, hidden, width), bf16),
            jax.ShapeDtypeStruct((tok_rows, width), bf16),
        ),
        in_specs=[whole] * 3,
        out_specs=(apart,) * 4,
        scratch_shapes=[dma((3 + chunks * n_tp,))],
        compiler_params=pltpu.CompilerParams(vmem_limit_bytes=8 * 1024 * 1024),
    )(in_mats, out_mat, rows)


def aligned(mesh, tokens, routes, gate_weight, down_weight):
    n_fs, n_tp = mesh.shape["fs"], mesh.shape["tp"]
    n = n_fs * n_tp
    tok_rows = tokens.shape[0] // n
    capacity = max(2, 3 * tok_rows * routes.shape[1] // (2 * n))
    return (
        gate_weight.shape[0] == n
        and n_fs % 4 == 0
        and n % 32 == 0
        and capacity % 8 == 0
        and tok_rows % 128 == 0
        and tokens.shape[1] % 512 == 0
        and gate_weight.shape[1] // n_fs % 128 == 0
        and gate_weight.shape[2] // n_tp % 128 == 0
        and down_weight.shape[1] // n_fs % 16 == 0
        and down_weight.shape[2] // n_tp % 128 == 0
    )


def solution(mesh):
    placed = (
        P(("fs", "tp"), None),
        P(("fs", "tp"), None),
        P(("fs", "tp"), None),
        P("fs"),
        P(None, "fs", "tp"),
        P(None, "fs", "tp"),
        P(None, "fs", "tp"),
    )

    def run(tokens, routes, route_weight, norm_gain, gate_weight, up_weight, down_weight):
        direct = aligned(mesh, tokens, routes, gate_weight, down_weight)
        return jax.shard_map(
            direct_shards if direct else shards,
            mesh=mesh,
            in_specs=placed,
            out_specs=(
                P(("fs", "tp"), None, None),
                P(("fs", "tp"), None, None),
                P(("fs", "tp"), None, None),
                P(("fs", "tp"), None),
            ),
            check_vma=False,
        )(tokens, routes, route_weight, norm_gain, gate_weight, up_weight, down_weight)

    return run
```

```python
import functools

import jax
import jax.numpy as jnp
from jax import lax
from jax.experimental import pallas as pl
from jax.experimental.pallas import tpu as pltpu
from jax.sharding import PartitionSpec as P

norm_epsilon = 1e-06
clamp_limit = 7.0
sigmoid_slope = 1.702
MESH = pl.DeviceIdType.MESH


def feed(inputs, gate_mat, up_mat, down_mat):
    gate_pre = jnp.dot(inputs, gate_mat, preferred_element_type=jnp.float32)
    up_pre = jnp.dot(inputs, up_mat, preferred_element_type=jnp.float32)
    gate_part = jnp.minimum(gate_pre, clamp_limit)
    linear_part = jnp.clip(up_pre, -clamp_limit, clamp_limit)
    activation = (
        gate_part * jax.nn.sigmoid(sigmoid_slope * gate_part) * (linear_part + 1.0)
    ).astype(jnp.bfloat16)
    return jnp.dot(activation, down_mat, preferred_element_type=jnp.float32).astype(jnp.bfloat16)


def assemble(received, rows_groups, column_groups):
    tile_rows = received.shape[2]
    tile_columns = received.shape[3]
    sources = received.reshape(rows_groups, column_groups, tile_rows, tile_columns)
    return sources.transpose(0, 2, 1, 3).reshape(
        1, rows_groups * tile_rows, column_groups * tile_columns
    )


def shards(tokens, routes, route_weight, norm_gain, gate_weight, up_weight, down_weight):
    gain_column = norm_gain[None, :, None]
    gate_tiles = (gate_weight * gain_column).astype(jnp.bfloat16)
    up_tiles = (up_weight * gain_column).astype(jnp.bfloat16)
    down_tiles = down_weight.astype(jnp.bfloat16)
    rows_groups = lax.axis_size("fs")
    column_groups = lax.axis_size("tp")
    arrived = (
        lax.all_to_all(gate_tiles[:, None], ("fs", "tp"), split_axis=0, concat_axis=1, tiled=True),
        lax.all_to_all(up_tiles[:, None], ("fs", "tp"), split_axis=0, concat_axis=1, tiled=True),
        lax.all_to_all(down_tiles[:, None], ("fs", "tp"), split_axis=0, concat_axis=1, tiled=True),
    )
    gate_new = assemble(arrived[0], rows_groups, column_groups)
    up_new = assemble(arrived[1], rows_groups, column_groups)
    down_new = assemble(arrived[2], rows_groups, column_groups)
    experts = rows_groups * column_groups
    tok_rows, model_width = tokens.shape
    per_token = routes.shape[1]
    capacity = max(2, 3 * tok_rows * per_token // (2 * experts))
    values = tokens.astype(jnp.float32)
    squares = jnp.mean(values * values, axis=1, keepdims=True)
    normed = (values * lax.rsqrt(squares + norm_epsilon)).astype(jnp.bfloat16)
    flat_routes = routes.reshape(-1)
    onehot = (flat_routes[:, None] == jnp.arange(experts, dtype=jnp.int32)[None, :]).astype(
        jnp.int32
    )
    earlier = jnp.cumsum(onehot, axis=0) - onehot
    rank = jnp.sum(earlier * onehot, axis=1)
    slot_index = flat_routes * capacity + rank
    slot_numbers = jnp.arange(experts * capacity, dtype=jnp.int32)
    select = jnp.any(
        slot_index.reshape(tok_rows, per_token)[None, :, :] == slot_numbers[:, None, None], axis=2
    )
    buffer = jnp.dot(
        select.astype(jnp.bfloat16), normed, preferred_element_type=jnp.float32
    ).astype(jnp.bfloat16)
    buffer = buffer.reshape(experts, 1, capacity, model_width)
    slot_rows = lax.all_to_all(buffer, ("fs", "tp"), split_axis=0, concat_axis=1, tiled=True)
    sources = slot_rows.shape[1]
    count = slot_rows.shape[2]
    expert_out = feed(slot_rows.reshape(-1, model_width), gate_new[0], up_new[0], down_new[0])
    expert_out = expert_out.reshape(1, sources, count, model_width)
    returned = lax.all_to_all(expert_out, ("fs", "tp"), split_axis=1, concat_axis=0, tiled=True)
    returned = returned.reshape(experts * capacity, model_width)
    picked = returned[slot_index].reshape(tok_rows, per_token, model_width)
    mixed = jnp.sum(picked.astype(jnp.float32) * route_weight[:, :, None], axis=1).astype(
        jnp.bfloat16
    )
    return (gate_new, up_new, down_new, mixed)


def exchange_kernel(
    sizes, tokens_far, routes_far, weight_far, gain_far, gate, up, down,
    in_mats, out_mat, mixed,
    tokens, routes_t, weight_t, gain, gate_in, up_in, down_in, gains, in_tiles, out_tiles,
    arrived, normed, slots_out, slots_in, active, far_routes, far_weight,
    mix_high, mix_low, rows_out, rows_in, side_out, side_in, totals, part_out, part_in,
    load_sem, token_send, token_recv, route_send, route_recv,
    first_send, first_recv, near_send, near_recv, slot_send, slot_recv,
    second_send, second_recv, back_send, back_recv, side_send, side_recv, part_send, part_recv, ready,
):
    n_fs, n_tp, capacity, splits = sizes
    n = n_fs * n_tp
    fs, tp = lax.axis_index("fs"), lax.axis_index("tp")
    tok_rows, width = tokens.shape
    tile_rows, tile_cols = gate_in.shape[1:]
    chunks, down_rows, lanes = out_tiles.shape[1:]
    down_cols = chunks * lanes
    block = n_tp * lanes
    per_token = routes_t.shape[0]

    planes = 4
    plane_fs = n_fs // planes
    plane = n // planes
    layer, place = fs // plane_fs, lax.rem(fs, plane_fs)
    spot = place * n_tp + tp

    def flip(turn):
        low = lax.rem(layer + turn, 2)
        high = lax.rem(layer // 2 + turn // 2, 2)
        return 2 * high + low

    def device(turn, shift):
        to_place = lax.rem(place + shift // n_tp, plane_fs)
        to_tp = lax.rem(tp + lax.rem(shift, n_tp), n_tp)
        return flip(turn) * plane_fs + to_place, to_tp, to_place * n_tp + to_tp

    def peer(step):
        paired = 1 - step // (n - 2)
        step = step + (1 - 2 * lax.rem(step, 2)) * paired * 0
        crossing = 1 - lax.rem(step, 2)
        at = lax.rem(step // 2 + 1 - crossing, n // 2)
        to_fs, to_tp, _ = device(2 * crossing + lax.rem(at, 2), at // 2)
        return to_fs, to_tp, to_fs * n_tp + to_tp

    def cross(at):
        to_fs, to_tp, _ = device(2 + lax.rem(at, 2), at // 2)
        return to_fs, to_tp, to_fs * n_tp + to_tp

    def close(at):
        at = lax.rem(at + 1, n // 2)
        to_fs, to_tp, _ = device(lax.rem(at, 2), at // 2)
        return to_fs, to_tp, to_fs * n_tp + to_tp

    def remote(source, target, send, recv, to):
        return pltpu.make_async_remote_copy(
            src_ref=source,
            dst_ref=target,
            send_sem=send,
            recv_sem=recv,
            device_id=(to[0], to[1]),
            device_id_type=MESH,
        )

    barrier = pltpu.get_barrier_semaphore()

    across = [device(turn, 0) for turn in range(1, planes)]
    aside = [device(0, shift) for shift in range(1, n_tp)]
    along = [device(0, shift * n_tp) for shift in range(1, plane_fs)]

    def greet(semaphore, group):
        for to in group:
            pl.semaphore_signal(semaphore, inc=1, device_id=(to[0], to[1]), device_id_type=MESH)

    loads = [
        pltpu.make_async_copy(source, target, load_sem.at[i])
        for i, (source, target) in enumerate(
            [
                (gain_far, gain),
                (routes_far, routes_t),
                (weight_far, weight_t),
                (tokens_far, tokens),
                (gate, gate_in),
                (up, up_in),
                (down, down_in),
            ]
        )
    ]
    for load in loads:
        load.start()
    greet(barrier, across + along + aside)

    for load in loads[:4]:
        load.wait()
    for i in range(tile_rows // lanes):
        gains[i * lanes : (i + 1) * lanes, :] = jnp.transpose(
            jnp.broadcast_to(gain[i : i + 1, :], (tile_cols, lanes))
        )

    def token_copy(turn, source):
        to = 1 if turn == 3 else turn
        return remote(
            source, arrived.at[turn - 1], token_send.at[turn - 1], token_recv.at[turn - 1], device(to, 0)
        )

    def route_copy(turn):
        return remote(
            routes_t, far_routes.at[turn - 1], route_send.at[turn - 1], route_recv.at[turn - 1], device(turn, 0)
        )

    def weight_copy(turn):
        return remote(
            weight_t, far_weight.at[turn - 1], route_send.at[turn + 2], route_recv.at[turn + 2], device(turn, 0)
        )

    token_copies = [
        token_copy(1, tokens),
        token_copy(2, tokens),
        token_copy(3, arrived.at[1]),
    ]
    route_copies = [copy(turn) for copy in (route_copy, weight_copy) for turn in (1, 2, 3)]

    def first_copy(to):
        return remote(
            in_tiles.at[to[2]],
            in_mats.at[
                :,
                pl.ds(pl.multiple_of(fs * tile_rows, tile_rows), tile_rows),
                pl.ds(pl.multiple_of(tp * tile_cols, tile_cols), tile_cols),
            ],
            first_send,
            first_recv,
            to,
        )

    own_rows = pl.ds(pl.multiple_of(fs * down_rows, down_rows), down_rows)
    own_lanes = pl.ds(pl.multiple_of(tp * lanes, lanes), lanes)

    def near_copy(to):
        return remote(
            out_tiles.at[to[2]], out_mat.at[:, own_rows, own_lanes], near_send, near_recv, to
        )

    def second_copy(c, to):
        return remote(
            out_tiles.at[to[2], c],
            out_mat.at[c, own_rows, own_lanes],
            second_send.at[c],
            second_recv.at[c],
            to,
        )

    def cast_first(step):
        e = peer(step)[2]
        in_tiles[e, 0] = (gate_in[e] * gains[...]).astype(jnp.bfloat16)
        in_tiles[e, 1] = (up_in[e] * gains[...]).astype(jnp.bfloat16)

    def cast_second(step):
        e = peer(step)[2]
        for c in range(chunks):
            out_tiles[e, c] = down_in[e, :, c * lanes : (c + 1) * lanes].astype(jnp.bfloat16)

    def send_first(step, carry):
        cast_first(step + 1)
        first_copy(peer(step)).start()
        return carry

    before = (
        lax.broadcasted_iota(jnp.int32, (tok_rows, tok_rows), 0)
        < lax.broadcasted_iota(jnp.int32, (tok_rows, tok_rows), 1)
    ).astype(jnp.float32).astype(jnp.bfloat16)

    experts = lax.broadcasted_iota(jnp.int32, (plane, tok_rows), 0) + layer * plane
    number = lax.broadcasted_iota(jnp.int32, (plane, capacity, tok_rows), 1).astype(jnp.float32)

    def named_in(paths, shares):
        named = jnp.zeros((plane, tok_rows), jnp.float32)
        scaled = jnp.zeros((plane, tok_rows), jnp.float32)
        for k in range(per_token):
            hit = paths[k : k + 1, :] == experts
            named = named + hit.astype(jnp.float32)
            if shares is not None:
                scaled = scaled + jnp.where(hit, shares[k : k + 1, :], 0.0)
        rank = jnp.dot(named.astype(jnp.bfloat16), before, preferred_element_type=jnp.float32)
        rank = jnp.where(named > 0.5, rank, -1.0)
        return (rank[:, None, :] == number).astype(jnp.float32), scaled

    def normalize(turn, rows_ref):
        values = rows_ref[...].astype(jnp.float32)
        squares = jnp.mean(values * values, axis=1, keepdims=True)
        normed[turn] = (values * lax.rsqrt(squares + norm_epsilon)).astype(jnp.bfloat16)

    def fill_slots(turn, paths):
        select, _ = named_in(paths, None)
        rows = jnp.dot(
            select.reshape(plane * capacity, tok_rows).astype(jnp.bfloat16),
            normed[turn],
            preferred_element_type=jnp.float32,
        )
        slots_out[:, turn] = rows.reshape(plane, capacity, width).astype(jnp.bfloat16)

    def fill_mix(turn, paths, shares):
        select, scaled = named_in(paths, shares)
        picks = jnp.transpose((select * scaled[:, None, :]).reshape(plane * capacity, tok_rows))
        high = picks.astype(jnp.bfloat16)
        mix_high[turn] = high
        mix_low[turn] = (picks - high.astype(jnp.float32)).astype(jnp.bfloat16)

    def slot_copy(turn, to):
        return remote(
            slots_out.at[to[2], turn], slots_in.at[spot, turn], slot_send, slot_recv, to
        )

    def send_slots(turn):
        def send_one(step, carry):
            slot_copy(turn, device(0, step)).start()
            return carry

        lax.fori_loop(1, plane, send_one, 0)
        slots_in[spot, turn] = slots_out[spot, turn]

    def send_some(start, stop):
        lax.fori_loop(start, stop, send_first, 0)

    normalize(0, tokens)
    pl.semaphore_wait(barrier, len(across + along + aside))
    greet(ready.at[0], aside)
    for each in route_copies:
        each.start()
    token_copies[1].start()
    token_copies[0].start()
    pl.semaphore_wait(ready.at[0], len(aside))
    greet(ready.at[1], along)
    fill_slots(0, routes_t)
    loads[4].wait()
    loads[5].wait()
    cast_first(0)
    pl.semaphore_wait(ready.at[1], len(along))
    send_some(0, n // 8)
    send_slots(0)
    send_some(n // 8, 3 * n // 8)
    for each in route_copies:
        each.wait_recv()
    token_copies[1].wait_recv()
    token_copies[2].start()
    normalize(2, arrived.at[1])
    fill_slots(2, far_routes.at[1])
    send_some(3 * n // 8, n // 2)
    send_slots(2)
    token_copies[0].wait_recv()
    normalize(1, arrived.at[0])
    fill_slots(1, far_routes.at[0])
    send_some(n // 2, 5 * n // 8)
    send_slots(1)
    token_copies[2].wait_recv()
    normalize(3, arrived.at[2])
    fill_slots(3, far_routes.at[2])
    send_some(5 * n // 8, 6 * n // 8)
    send_slots(3)
    send_some(6 * n // 8, n - 1)

    me = fs * n_tp + tp
    mine_rows = pl.ds(pl.multiple_of(fs * tile_rows, tile_rows), tile_rows)
    mine_cols = pl.ds(pl.multiple_of(tp * tile_cols, tile_cols), tile_cols)
    in_mats[0, mine_rows, mine_cols] = in_tiles[me, 0]
    in_mats[1, mine_rows, mine_cols] = in_tiles[me, 1]

    loads[6].wait()
    cast_second(0)
    cast_second(1)

    def send_second(step, carry):
        cast_second(2 * step + 2)
        cast_second(2 * step + 3)
        second_copy(0, cross(step)).start()
        return carry

    lax.fori_loop(0, n // 2 - 1, send_second, 0)
    second_copy(0, cross(n // 2 - 1)).start()

    def send_near(step, carry):
        near_copy(close(step)).start()
        return carry

    lax.fori_loop(0, n // 2 - 1, send_near, 0)
    out_mat[:, own_rows, own_lanes] = out_tiles[me]

    def send_chunk(c):
        def send_one(step, carry):
            second_copy(c, cross(step)).start()
            return carry

        lax.fori_loop(0, n // 2, send_one, 0)

    send_chunk(1)
    fill_mix(0, routes_t, weight_t)
    for turn in range(1, planes):
        fill_mix(turn, far_routes.at[turn - 1], far_weight.at[turn - 1])

    near = device(1, 0)

    def take(size_ref, send, recv):
        return remote(size_ref, size_ref, send, recv, near)

    slots_all = take(slots_in.at[pl.ds(0, plane - 1)], slot_send, slot_recv)
    first_all = take(in_tiles.at[pl.ds(0, n - 1)], first_send, first_recv)
    near_all = take(out_tiles.at[pl.ds(0, n // 2 - 1)], near_send, near_recv)

    def second_all(c):
        return take(out_tiles.at[pl.ds(0, n // 2), c], second_send.at[c], second_recv.at[c])

    bounds = [
        (c, i * block // parts, (i + 1) * block // parts)
        for c, parts in enumerate(splits)
        for i in range(parts)
    ]
    pieces = len(bounds)

    def back_all(j):
        c, start, stop = bounds[j]
        rows = rows_in.at[c, pl.ds(0, plane - 1), :, :, start:stop]
        return take(rows, back_send.at[j], back_recv.at[j])

    slots_all.wait_recv()
    first_all.wait_recv()

    group = active.shape[1]
    held = group // (planes * capacity)

    def activate(g, carry):
        inputs = slots_in[pl.ds(g * held, held)].astype(jnp.float32)
        inputs = inputs.reshape(group, width).astype(jnp.bfloat16)
        gate_pre = jnp.dot(inputs, in_mats[0], preferred_element_type=jnp.float32)
        up_pre = jnp.dot(inputs, in_mats[1], preferred_element_type=jnp.float32)
        gate_part = jnp.minimum(gate_pre, clamp_limit)
        linear_part = jnp.clip(up_pre, -clamp_limit, clamp_limit)
        active[g] = (
            gate_part * jax.nn.sigmoid(sigmoid_slope * gate_part) * (linear_part + 1.0)
        ).astype(jnp.bfloat16)
        return carry

    lax.fori_loop(0, active.shape[0], activate, 0)
    near_all.wait_recv()

    def back_copy(j, shift):
        to = device(0, shift)
        c, start, stop = bounds[j]
        return remote(
            rows_out.at[c, to[2], :, :, start:stop],
            rows_in.at[c, spot, :, :, start:stop],
            back_send.at[j],
            back_recv.at[j],
            to,
        )

    def side_copy(j):
        c, start, stop = bounds[j]
        return remote(
            side_out.at[c, :, :, start:stop],
            side_in.at[c, :, :, start:stop],
            side_send.at[j],
            side_recv.at[j],
            device(1, 0),
        )

    def part_copy(j):
        c, start, stop = bounds[j]
        return remote(
            part_out.at[c, :, start:stop],
            part_in.at[c, :, start:stop],
            part_send.at[j],
            part_recv.at[j],
            device(2, 0),
        )

    def project(c):
        second_all(c).wait_recv()
        for j in of_chunk(c):
            cols = slice(*bounds[j][1:])

            def project_group(g, carry):
                rows = jnp.dot(
                    active[g], out_mat[c, :, cols], preferred_element_type=jnp.float32
                )
                rows_out[c, pl.ds(g * held, held), :, :, cols] = rows.reshape(
                    held, planes, capacity, cols.stop - cols.start
                ).astype(jnp.bfloat16)
                return carry

            lax.fori_loop(0, active.shape[0], project_group, 0)

            def send_back(step, carry):
                back_copy(j, step).start()
                return carry

            lax.fori_loop(1, plane, send_back, 0)
            rows_in[c, spot, :, :, cols] = rows_out[c, spot, :, :, cols]

    span = plane * capacity

    def combine(j, turn):
        c, start, stop = bounds[j]
        rows = rows_in[c, :, turn, :, start:stop].astype(jnp.float32)
        rows = rows.reshape(span, stop - start).astype(jnp.bfloat16)
        total = jnp.dot(mix_high[turn], rows, preferred_element_type=jnp.float32)
        return total + jnp.dot(mix_low[turn], rows, preferred_element_type=jnp.float32)

    def give_side(j):
        c, start, stop = bounds[j]
        back_all(j).wait_recv()
        for q in range(2):
            side_out[c, q, :, start:stop] = combine(j, 2 * q + 1).astype(jnp.bfloat16)
        for q in range(1, -1, -1):
            totals[c, q, :, start:stop] = combine(j, 2 * q)
            if q == 1:
                side_copy(j).start()

    def give_part(j):
        c, start, stop = bounds[j]
        cols = slice(start, stop)
        side_copy(j).wait_recv()
        part_out[c, :, cols] = (
            totals[c, 1, :, cols] + side_in[c, 1, :, cols].astype(jnp.float32)
        ).astype(jnp.bfloat16)
        totals[c, 0, :, cols] = totals[c, 0, :, cols] + side_in[c, 0, :, cols].astype(jnp.float32)
        part_copy(j).start()

    def finish(j):
        c, start, stop = bounds[j]
        part_copy(j).wait_recv()
        total = totals[c, 0, :, start:stop] + part_in[c, :, start:stop].astype(jnp.float32)
        total = total.astype(jnp.bfloat16)
        for k in range(start // lanes, stop // lanes):
            left = k * down_cols + c * lanes
            mixed[:, left : left + lanes] = total[:, k * lanes - start : (k + 1) * lanes - start]

    def of_chunk(c):
        return [j for j in range(pieces) if bounds[j][0] == c]

    def run(stage, c):
        for j in of_chunk(c):
            stage(j)

    for c in range(chunks):
        project(c)
        if c > 0:
            run(give_side, c - 1)
        if c + 2 < chunks:
            send_chunk(c + 2)
        if c > 1:
            run(give_part, c - 2)
    last = of_chunk(chunks - 1)
    give_side(last[0])
    run(give_part, chunks - 2)
    for j in last[1:]:
        give_side(j)
    for j in last:
        give_part(j)
    for j in range(pieces):
        finish(j)

    first_all.wait_send()
    near_all.wait_send()
    slots_all.wait_send()
    for c in range(chunks):
        second_all(c).wait_send()
    for j in range(pieces):
        back_all(j).wait_send()
        side_copy(j).wait_send()
        part_copy(j).wait_send()
    for each in token_copies + route_copies:
        each.wait_send()


def keep_kernel(in_mats, out_mat, rows, gate_out, up_out, down_out, mixed, sem):
    chunks, _, block = out_mat.shape
    n_tp = block // 128
    lanes = block // n_tp
    down_cols = chunks * lanes
    copies = [
        (in_mats.at[0], gate_out.at[0]),
        (in_mats.at[1], up_out.at[0]),
        (rows, mixed),
    ]
    for c in range(chunks):
        for k in range(n_tp):
            start = k * down_cols + c * lanes
            copies.append(
                (
                    out_mat.at[c, :, k * lanes : (k + 1) * lanes],
                    down_out.at[0, :, start : start + lanes],
                )
            )
    copies = [
        pltpu.make_async_copy(source, target, sem.at[i])
        for i, (source, target) in enumerate(copies)
    ]
    for copy in copies:
        copy.start()
    for copy in copies:
        copy.wait()


def direct_shards(
    tokens, routes, route_weight, norm_gain, gate_weight, up_weight, down_weight
):
    n_fs, n_tp = lax.axis_size("fs"), lax.axis_size("tp")
    n = n_fs * n_tp
    tok_rows, width = tokens.shape
    tile_rows, tile_cols = gate_weight.shape[1:]
    down_rows, down_cols = down_weight.shape[1:]
    hidden = n_tp * tile_cols
    lanes = 128
    chunks = down_cols // lanes
    block = n_tp * lanes
    plane = n // 4
    splits = (2,) * chunks
    pieces = sum(splits)
    per_token = routes.shape[1]
    capacity = max(2, 3 * tok_rows * per_token // (2 * n))
    bf16, f32 = jnp.bfloat16, jnp.float32
    whole = pl.BlockSpec(memory_space=pltpu.VMEM)
    apart = pl.BlockSpec(memory_space=pltpu.HBM)
    dma = pltpu.SemaphoreType.DMA
    groups = 4
    in_mats, out_mat, rows = pl.pallas_call(
        functools.partial(exchange_kernel, (n_fs, n_tp, capacity, splits)),
        out_shape=(
            pltpu.VMEM((2, width, hidden), bf16),
            pltpu.VMEM((chunks, hidden, block), bf16),
            pltpu.VMEM((tok_rows, width), bf16),
        ),
        in_specs=[apart] * 7,
        out_specs=(whole, whole, whole),
        scratch_shapes=[
            pltpu.VMEM((tok_rows, width), tokens.dtype),
            pltpu.VMEM((per_token, tok_rows), routes.dtype),
            pltpu.VMEM((per_token, tok_rows), f32),
            pltpu.VMEM((tile_rows // lanes, lanes), f32),
            pltpu.VMEM((n, tile_rows, tile_cols), f32),
            pltpu.VMEM((n, tile_rows, tile_cols), f32),
            pltpu.VMEM((n, down_rows, down_cols), f32),
            pltpu.VMEM((tile_rows, tile_cols), f32),
            pltpu.VMEM((n, 2, tile_rows, tile_cols), bf16),
            pltpu.VMEM((n, chunks, down_rows, lanes), bf16),
            pltpu.VMEM((3, tok_rows, width), bf16),
            pltpu.VMEM((4, tok_rows, width), bf16),
            pltpu.VMEM((plane, 4, capacity, width), bf16),
            pltpu.VMEM((plane, 4, capacity, width), bf16),
            pltpu.VMEM((groups, n * capacity // groups, hidden), bf16),
            pltpu.VMEM((3, per_token, tok_rows), routes.dtype),
            pltpu.VMEM((3, per_token, tok_rows), f32),
            pltpu.VMEM((4, tok_rows, plane * capacity), bf16),
            pltpu.VMEM((4, tok_rows, plane * capacity), bf16),
            pltpu.VMEM((chunks, plane, 4, capacity, block), bf16),
            pltpu.VMEM((chunks, plane, 4, capacity, block), bf16),
            pltpu.VMEM((chunks, 2, tok_rows, block), bf16),
            pltpu.VMEM((chunks, 2, tok_rows, block), bf16),
            pltpu.VMEM((chunks, 2, tok_rows, block), f32),
            pltpu.VMEM((chunks, tok_rows, block), bf16),
            pltpu.VMEM((chunks, tok_rows, block), bf16),
            dma((7,)),
            dma((3,)),
            dma((3,)),
            dma((6,)),
            dma((6,)),
            dma,
            dma,
            dma,
            dma,
            dma,
            dma,
        ]
        + [dma((chunks,))] * 2
        + [dma((pieces,))] * 6
        + [pltpu.SemaphoreType.REGULAR((2,))],
        compiler_params=pltpu.CompilerParams(
            collective_id=0, has_side_effects=True, vmem_limit_bytes=52 * 1024 * 1024
        ),
    )(
        tokens,
        routes.T,
        route_weight.T,
        norm_gain.reshape(tile_rows // lanes, lanes),
        gate_weight,
        up_weight,
        down_weight,
    )
    return pl.pallas_call(
        keep_kernel,
        out_shape=(
            jax.ShapeDtypeStruct((1, width, hidden), bf16),
            jax.ShapeDtypeStruct((1, width, hidden), bf16),
            jax.ShapeDtypeStruct((1, hidden, width), bf16),
            jax.ShapeDtypeStruct((tok_rows, width), bf16),
        ),
        in_specs=[whole] * 3,
        out_specs=(apart,) * 4,
        scratch_shapes=[dma((3 + chunks * n_tp,))],
        compiler_params=pltpu.CompilerParams(vmem_limit_bytes=8 * 1024 * 1024),
    )(in_mats, out_mat, rows)


def aligned(mesh, tokens, routes, gate_weight, down_weight):
    n_fs, n_tp = mesh.shape["fs"], mesh.shape["tp"]
    n = n_fs * n_tp
    tok_rows = tokens.shape[0] // n
    capacity = max(2, 3 * tok_rows * routes.shape[1] // (2 * n))
    return (
        gate_weight.shape[0] == n
        and n_fs % 4 == 0
        and n % 32 == 0
        and capacity % 8 == 0
        and tok_rows % 128 == 0
        and tokens.shape[1] % 512 == 0
        and gate_weight.shape[1] // n_fs % 128 == 0
        and gate_weight.shape[2] // n_tp % 128 == 0
        and down_weight.shape[1] // n_fs % 16 == 0
        and down_weight.shape[2] // n_tp % 128 == 0
    )


def solution(mesh):
    placed = (
        P(("fs", "tp"), None),
        P(("fs", "tp"), None),
        P(("fs", "tp"), None),
        P("fs"),
        P(None, "fs", "tp"),
        P(None, "fs", "tp"),
        P(None, "fs", "tp"),
    )

    def run(tokens, routes, route_weight, norm_gain, gate_weight, up_weight, down_weight):
        direct = aligned(mesh, tokens, routes, gate_weight, down_weight)
        return jax.shard_map(
            direct_shards if direct else shards,
            mesh=mesh,
            in_specs=placed,
            out_specs=(
                P(("fs", "tp"), None, None),
                P(("fs", "tp"), None, None),
                P(("fs", "tp"), None, None),
                P(("fs", "tp"), None),
            ),
            check_vma=False,
        )(tokens, routes, route_weight, norm_gain, gate_weight, up_weight, down_weight)

    return run
```

```python
import functools

import jax
import jax.numpy as jnp
from jax import lax
from jax.experimental import pallas as pl
from jax.experimental.pallas import tpu as pltpu
from jax.sharding import PartitionSpec as P

norm_epsilon = 1e-06
clamp_limit = 7.0
sigmoid_slope = 1.702
MESH = pl.DeviceIdType.MESH


def feed(inputs, gate_mat, up_mat, down_mat):
    gate_pre = jnp.dot(inputs, gate_mat, preferred_element_type=jnp.float32)
    up_pre = jnp.dot(inputs, up_mat, preferred_element_type=jnp.float32)
    gate_part = jnp.minimum(gate_pre, clamp_limit)
    linear_part = jnp.clip(up_pre, -clamp_limit, clamp_limit)
    activation = (
        gate_part * jax.nn.sigmoid(sigmoid_slope * gate_part) * (linear_part + 1.0)
    ).astype(jnp.bfloat16)
    return jnp.dot(activation, down_mat, preferred_element_type=jnp.float32).astype(jnp.bfloat16)


def assemble(received, rows_groups, column_groups):
    tile_rows = received.shape[2]
    tile_columns = received.shape[3]
    sources = received.reshape(rows_groups, column_groups, tile_rows, tile_columns)
    return sources.transpose(0, 2, 1, 3).reshape(
        1, rows_groups * tile_rows, column_groups * tile_columns
    )


def shards(tokens, routes, route_weight, norm_gain, gate_weight, up_weight, down_weight):
    gain_column = norm_gain[None, :, None]
    gate_tiles = (gate_weight * gain_column).astype(jnp.bfloat16)
    up_tiles = (up_weight * gain_column).astype(jnp.bfloat16)
    down_tiles = down_weight.astype(jnp.bfloat16)
    rows_groups = lax.axis_size("fs")
    column_groups = lax.axis_size("tp")
    arrived = (
        lax.all_to_all(gate_tiles[:, None], ("fs", "tp"), split_axis=0, concat_axis=1, tiled=True),
        lax.all_to_all(up_tiles[:, None], ("fs", "tp"), split_axis=0, concat_axis=1, tiled=True),
        lax.all_to_all(down_tiles[:, None], ("fs", "tp"), split_axis=0, concat_axis=1, tiled=True),
    )
    gate_new = assemble(arrived[0], rows_groups, column_groups)
    up_new = assemble(arrived[1], rows_groups, column_groups)
    down_new = assemble(arrived[2], rows_groups, column_groups)
    experts = rows_groups * column_groups
    tok_rows, model_width = tokens.shape
    per_token = routes.shape[1]
    capacity = max(2, 3 * tok_rows * per_token // (2 * experts))
    values = tokens.astype(jnp.float32)
    squares = jnp.mean(values * values, axis=1, keepdims=True)
    normed = (values * lax.rsqrt(squares + norm_epsilon)).astype(jnp.bfloat16)
    flat_routes = routes.reshape(-1)
    onehot = (flat_routes[:, None] == jnp.arange(experts, dtype=jnp.int32)[None, :]).astype(
        jnp.int32
    )
    earlier = jnp.cumsum(onehot, axis=0) - onehot
    rank = jnp.sum(earlier * onehot, axis=1)
    slot_index = flat_routes * capacity + rank
    slot_numbers = jnp.arange(experts * capacity, dtype=jnp.int32)
    select = jnp.any(
        slot_index.reshape(tok_rows, per_token)[None, :, :] == slot_numbers[:, None, None], axis=2
    )
    buffer = jnp.dot(
        select.astype(jnp.bfloat16), normed, preferred_element_type=jnp.float32
    ).astype(jnp.bfloat16)
    buffer = buffer.reshape(experts, 1, capacity, model_width)
    slot_rows = lax.all_to_all(buffer, ("fs", "tp"), split_axis=0, concat_axis=1, tiled=True)
    sources = slot_rows.shape[1]
    count = slot_rows.shape[2]
    expert_out = feed(slot_rows.reshape(-1, model_width), gate_new[0], up_new[0], down_new[0])
    expert_out = expert_out.reshape(1, sources, count, model_width)
    returned = lax.all_to_all(expert_out, ("fs", "tp"), split_axis=1, concat_axis=0, tiled=True)
    returned = returned.reshape(experts * capacity, model_width)
    picked = returned[slot_index].reshape(tok_rows, per_token, model_width)
    mixed = jnp.sum(picked.astype(jnp.float32) * route_weight[:, :, None], axis=1).astype(
        jnp.bfloat16
    )
    return (gate_new, up_new, down_new, mixed)


def exchange_kernel(
    sizes, tokens_far, routes_far, weight_far, gain_far, gate, up, down,
    in_mats, out_mat, mixed,
    tokens, routes_t, weight_t, gain, gate_in, up_in, down_in, gains, in_tiles, out_tiles,
    arrived, normed, slots_out, slots_in, active, far_routes, far_weight,
    mix_high, mix_low, rows_out, rows_in, side_out, side_in, totals, part_out, part_in,
    load_sem, token_send, token_recv, route_send, route_recv,
    first_send, first_recv, near_send, near_recv, slot_send, slot_recv,
    second_send, second_recv, back_send, back_recv, side_send, side_recv, part_send, part_recv, ready,
):
    n_fs, n_tp, capacity, splits = sizes
    n = n_fs * n_tp
    fs, tp = lax.axis_index("fs"), lax.axis_index("tp")
    tok_rows, width = tokens.shape
    tile_rows, tile_cols = gate_in.shape[1:]
    chunks, down_rows, lanes = out_tiles.shape[1:]
    down_cols = chunks * lanes
    block = n_tp * lanes
    per_token = routes_t.shape[0]

    planes = 4
    plane_fs = n_fs // planes
    plane = n // planes
    layer, place = fs // plane_fs, lax.rem(fs, plane_fs)
    spot = place * n_tp + tp

    def flip(turn):
        low = lax.rem(layer + turn, 2)
        high = lax.rem(layer // 2 + turn // 2, 2)
        return 2 * high + low

    def device(turn, shift):
        to_place = lax.rem(place + shift // n_tp, plane_fs)
        to_tp = lax.rem(tp + lax.rem(shift, n_tp), n_tp)
        return flip(turn) * plane_fs + to_place, to_tp, to_place * n_tp + to_tp

    def peer(step):
        paired = 1 - step // (n - 2)
        step = step + (1 - 2 * lax.rem(step, 2)) * paired * 0
        crossing = 1 - lax.rem(step, 2)
        at = lax.rem(step // 2 + 1 - crossing, n // 2)
        to_fs, to_tp, _ = device(2 * crossing + lax.rem(at, 2), at // 2)
        return to_fs, to_tp, to_fs * n_tp + to_tp

    def cross(at):
        to_fs, to_tp, _ = device(2 + lax.rem(at, 2), at // 2)
        return to_fs, to_tp, to_fs * n_tp + to_tp

    def close(at):
        at = lax.rem(at + 1, n // 2)
        to_fs, to_tp, _ = device(lax.rem(at, 2), at // 2)
        return to_fs, to_tp, to_fs * n_tp + to_tp

    def remote(source, target, send, recv, to):
        return pltpu.make_async_remote_copy(
            src_ref=source,
            dst_ref=target,
            send_sem=send,
            recv_sem=recv,
            device_id=(to[0], to[1]),
            device_id_type=MESH,
        )

    barrier = pltpu.get_barrier_semaphore()

    across = [device(turn, 0) for turn in range(1, planes)]
    aside = [device(0, shift) for shift in range(1, n_tp)]
    along = [device(0, shift * n_tp) for shift in range(1, plane_fs)]

    def greet(semaphore, group):
        for to in group:
            pl.semaphore_signal(semaphore, inc=1, device_id=(to[0], to[1]), device_id_type=MESH)

    loads = [
        pltpu.make_async_copy(source, target, load_sem.at[i])
        for i, (source, target) in enumerate(
            [
                (gain_far, gain),
                (routes_far, routes_t),
                (weight_far, weight_t),
                (tokens_far, tokens),
                (gate, gate_in),
                (up, up_in),
                (down, down_in),
            ]
        )
    ]
    for load in loads:
        load.start()
    greet(barrier, across + along + aside)

    for load in loads[:4]:
        load.wait()
    for i in range(tile_rows // lanes):
        gains[i * lanes : (i + 1) * lanes, :] = jnp.transpose(
            jnp.broadcast_to(gain[i : i + 1, :], (tile_cols, lanes))
        )

    def token_copy(turn, source):
        to = 1 if turn == 3 else turn
        return remote(
            source, arrived.at[turn - 1], token_send.at[turn - 1], token_recv.at[turn - 1], device(to, 0)
        )

    def route_copy(turn):
        return remote(
            routes_t, far_routes.at[turn - 1], route_send.at[turn - 1], route_recv.at[turn - 1], device(turn, 0)
        )

    def weight_copy(turn):
        return remote(
            weight_t, far_weight.at[turn - 1], route_send.at[turn + 2], route_recv.at[turn + 2], device(turn, 0)
        )

    token_copies = [
        token_copy(1, tokens),
        token_copy(2, tokens),
        token_copy(3, arrived.at[1]),
    ]
    route_copies = [copy(turn) for copy in (route_copy, weight_copy) for turn in (1, 2, 3)]

    def first_copy(to):
        return remote(
            in_tiles.at[to[2]],
            in_mats.at[
                :,
                pl.ds(pl.multiple_of(fs * tile_rows, tile_rows), tile_rows),
                pl.ds(pl.multiple_of(tp * tile_cols, tile_cols), tile_cols),
            ],
            first_send,
            first_recv,
            to,
        )

    own_rows = pl.ds(pl.multiple_of(fs * down_rows, down_rows), down_rows)
    own_lanes = pl.ds(pl.multiple_of(tp * lanes, lanes), lanes)

    def near_copy(to):
        return remote(
            out_tiles.at[to[2]], out_mat.at[:, own_rows, own_lanes], near_send, near_recv, to
        )

    def second_copy(c, to):
        return remote(
            out_tiles.at[to[2], c],
            out_mat.at[c, own_rows, own_lanes],
            second_send.at[c],
            second_recv.at[c],
            to,
        )

    def cast_first(step):
        e = peer(step)[2]
        in_tiles[e, 0] = (gate_in[e] * gains[...]).astype(jnp.bfloat16)
        in_tiles[e, 1] = (up_in[e] * gains[...]).astype(jnp.bfloat16)

    def cast_second(step):
        e = peer(step)[2]
        for c in range(chunks):
            out_tiles[e, c] = down_in[e, :, c * lanes : (c + 1) * lanes].astype(jnp.bfloat16)

    def send_first(step, carry):
        cast_first(step + 1)
        first_copy(peer(step)).start()
        return carry

    before = (
        lax.broadcasted_iota(jnp.int32, (tok_rows, tok_rows), 0)
        < lax.broadcasted_iota(jnp.int32, (tok_rows, tok_rows), 1)
    ).astype(jnp.float32).astype(jnp.bfloat16)

    experts = lax.broadcasted_iota(jnp.int32, (plane, tok_rows), 0) + layer * plane
    number = lax.broadcasted_iota(jnp.int32, (plane, capacity, tok_rows), 1).astype(jnp.float32)

    def named_in(paths, shares):
        named = jnp.zeros((plane, tok_rows), jnp.float32)
        scaled = jnp.zeros((plane, tok_rows), jnp.float32)
        for k in range(per_token):
            hit = paths[k : k + 1, :] == experts
            named = named + hit.astype(jnp.float32)
            if shares is not None:
                scaled = scaled + jnp.where(hit, shares[k : k + 1, :], 0.0)
        rank = jnp.dot(named.astype(jnp.bfloat16), before, preferred_element_type=jnp.float32)
        rank = jnp.where(named > 0.5, rank, -1.0)
        return (rank[:, None, :] == number).astype(jnp.float32), scaled

    def normalize(turn, rows_ref):
        values = rows_ref[...].astype(jnp.float32)
        squares = jnp.mean(values * values, axis=1, keepdims=True)
        normed[turn] = (values * lax.rsqrt(squares + norm_epsilon)).astype(jnp.bfloat16)

    def fill_slots(turn, paths):
        select, _ = named_in(paths, None)
        rows = jnp.dot(
            select.reshape(plane * capacity, tok_rows).astype(jnp.bfloat16),
            normed[turn],
            preferred_element_type=jnp.float32,
        )
        slots_out[:, turn] = rows.reshape(plane, capacity, width).astype(jnp.bfloat16)

    def fill_mix(turn, paths, shares):
        select, scaled = named_in(paths, shares)
        picks = jnp.transpose((select * scaled[:, None, :]).reshape(plane * capacity, tok_rows))
        high = picks.astype(jnp.bfloat16)
        mix_high[turn] = high
        mix_low[turn] = (picks - high.astype(jnp.float32)).astype(jnp.bfloat16)

    def slot_copy(turn, to):
        return remote(
            slots_out.at[to[2], turn], slots_in.at[spot, turn], slot_send, slot_recv, to
        )

    def send_slots(turn):
        def send_one(step, carry):
            slot_copy(turn, device(0, step)).start()
            return carry

        lax.fori_loop(1, plane, send_one, 0)
        slots_in[spot, turn] = slots_out[spot, turn]

    def send_some(start, stop):
        lax.fori_loop(start, stop, send_first, 0)

    normalize(0, tokens)
    pl.semaphore_wait(barrier, len(across + along + aside))
    greet(ready.at[0], aside)
    for each in route_copies:
        each.start()
    token_copies[1].start()
    token_copies[0].start()
    pl.semaphore_wait(ready.at[0], len(aside))
    greet(ready.at[1], along)
    loads[4].wait()
    loads[5].wait()
    cast_first(0)
    pl.semaphore_wait(ready.at[1], len(along))
    send_some(0, n // 8)
    fill_slots(0, routes_t)
    send_slots(0)
    send_some(n // 8, 3 * n // 8)
    for each in route_copies:
        each.wait_recv()
    token_copies[1].wait_recv()
    token_copies[2].start()
    normalize(2, arrived.at[1])
    fill_slots(2, far_routes.at[1])
    send_some(3 * n // 8, n // 2)
    send_slots(2)
    token_copies[0].wait_recv()
    normalize(1, arrived.at[0])
    fill_slots(1, far_routes.at[0])
    send_some(n // 2, 5 * n // 8)
    send_slots(1)
    token_copies[2].wait_recv()
    normalize(3, arrived.at[2])
    fill_slots(3, far_routes.at[2])
    send_some(5 * n // 8, 6 * n // 8)
    send_slots(3)
    send_some(6 * n // 8, n - 1)

    me = fs * n_tp + tp
    mine_rows = pl.ds(pl.multiple_of(fs * tile_rows, tile_rows), tile_rows)
    mine_cols = pl.ds(pl.multiple_of(tp * tile_cols, tile_cols), tile_cols)
    in_mats[0, mine_rows, mine_cols] = in_tiles[me, 0]
    in_mats[1, mine_rows, mine_cols] = in_tiles[me, 1]

    loads[6].wait()
    cast_second(0)
    cast_second(1)

    def send_second(step, carry):
        cast_second(2 * step + 2)
        cast_second(2 * step + 3)
        second_copy(0, cross(step)).start()
        return carry

    lax.fori_loop(0, n // 2 - 1, send_second, 0)
    second_copy(0, cross(n // 2 - 1)).start()

    def send_near(step, carry):
        near_copy(close(step)).start()
        return carry

    lax.fori_loop(0, n // 2 - 1, send_near, 0)
    out_mat[:, own_rows, own_lanes] = out_tiles[me]

    def send_chunk(c):
        def send_one(step, carry):
            second_copy(c, cross(step)).start()
            return carry

        lax.fori_loop(0, n // 2, send_one, 0)

    send_chunk(1)
    fill_mix(0, routes_t, weight_t)
    for turn in range(1, planes):
        fill_mix(turn, far_routes.at[turn - 1], far_weight.at[turn - 1])

    near = device(1, 0)

    def take(size_ref, send, recv):
        return remote(size_ref, size_ref, send, recv, near)

    slots_all = take(slots_in.at[pl.ds(0, plane - 1)], slot_send, slot_recv)
    first_all = take(in_tiles.at[pl.ds(0, n - 1)], first_send, first_recv)
    near_all = take(out_tiles.at[pl.ds(0, n // 2 - 1)], near_send, near_recv)

    def second_all(c):
        return take(out_tiles.at[pl.ds(0, n // 2), c], second_send.at[c], second_recv.at[c])

    bounds = [
        (c, i * block // parts, (i + 1) * block // parts)
        for c, parts in enumerate(splits)
        for i in range(parts)
    ]
    pieces = len(bounds)

    def back_all(j):
        c, start, stop = bounds[j]
        rows = rows_in.at[c, pl.ds(0, plane - 1), :, :, start:stop]
        return take(rows, back_send.at[j], back_recv.at[j])

    slots_all.wait_recv()
    first_all.wait_recv()

    group = active.shape[1]
    held = group // (planes * capacity)

    def activate(g, carry):
        inputs = slots_in[pl.ds(g * held, held)].astype(jnp.float32)
        inputs = inputs.reshape(group, width).astype(jnp.bfloat16)
        gate_pre = jnp.dot(inputs, in_mats[0], preferred_element_type=jnp.float32)
        up_pre = jnp.dot(inputs, in_mats[1], preferred_element_type=jnp.float32)
        gate_part = jnp.minimum(gate_pre, clamp_limit)
        linear_part = jnp.clip(up_pre, -clamp_limit, clamp_limit)
        active[g] = (
            gate_part * jax.nn.sigmoid(sigmoid_slope * gate_part) * (linear_part + 1.0)
        ).astype(jnp.bfloat16)
        return carry

    lax.fori_loop(0, active.shape[0], activate, 0)
    near_all.wait_recv()

    def back_copy(j, shift):
        to = device(0, shift)
        c, start, stop = bounds[j]
        return remote(
            rows_out.at[c, to[2], :, :, start:stop],
            rows_in.at[c, spot, :, :, start:stop],
            back_send.at[j],
            back_recv.at[j],
            to,
        )

    def side_copy(j):
        c, start, stop = bounds[j]
        return remote(
            side_out.at[c, :, :, start:stop],
            side_in.at[c, :, :, start:stop],
            side_send.at[j],
            side_recv.at[j],
            device(1, 0),
        )

    def part_copy(j):
        c, start, stop = bounds[j]
        return remote(
            part_out.at[c, :, start:stop],
            part_in.at[c, :, start:stop],
            part_send.at[j],
            part_recv.at[j],
            device(2, 0),
        )

    def project(c):
        second_all(c).wait_recv()
        for j in of_chunk(c):
            cols = slice(*bounds[j][1:])

            def project_group(g, carry):
                rows = jnp.dot(
                    active[g], out_mat[c, :, cols], preferred_element_type=jnp.float32
                )
                rows_out[c, pl.ds(g * held, held), :, :, cols] = rows.reshape(
                    held, planes, capacity, cols.stop - cols.start
                ).astype(jnp.bfloat16)
                return carry

            lax.fori_loop(0, active.shape[0], project_group, 0)

            def send_back(step, carry):
                back_copy(j, step).start()
                return carry

            lax.fori_loop(1, plane, send_back, 0)
            rows_in[c, spot, :, :, cols] = rows_out[c, spot, :, :, cols]

    span = plane * capacity

    def combine(j, turn):
        c, start, stop = bounds[j]
        rows = rows_in[c, :, turn, :, start:stop].astype(jnp.float32)
        rows = rows.reshape(span, stop - start).astype(jnp.bfloat16)
        total = jnp.dot(mix_high[turn], rows, preferred_element_type=jnp.float32)
        return total + jnp.dot(mix_low[turn], rows, preferred_element_type=jnp.float32)

    def give_side(j):
        c, start, stop = bounds[j]
        back_all(j).wait_recv()
        for q in range(2):
            side_out[c, q, :, start:stop] = combine(j, 2 * q + 1).astype(jnp.bfloat16)
        for q in range(1, -1, -1):
            totals[c, q, :, start:stop] = combine(j, 2 * q)
            if q == 1:
                side_copy(j).start()

    def give_part(j):
        c, start, stop = bounds[j]
        cols = slice(start, stop)
        side_copy(j).wait_recv()
        part_out[c, :, cols] = (
            totals[c, 1, :, cols] + side_in[c, 1, :, cols].astype(jnp.float32)
        ).astype(jnp.bfloat16)
        totals[c, 0, :, cols] = totals[c, 0, :, cols] + side_in[c, 0, :, cols].astype(jnp.float32)
        part_copy(j).start()

    def finish(j):
        c, start, stop = bounds[j]
        part_copy(j).wait_recv()
        total = totals[c, 0, :, start:stop] + part_in[c, :, start:stop].astype(jnp.float32)
        total = total.astype(jnp.bfloat16)
        for k in range(start // lanes, stop // lanes):
            left = k * down_cols + c * lanes
            mixed[:, left : left + lanes] = total[:, k * lanes - start : (k + 1) * lanes - start]

    def of_chunk(c):
        return [j for j in range(pieces) if bounds[j][0] == c]

    def run(stage, c):
        for j in of_chunk(c):
            stage(j)

    for c in range(chunks):
        project(c)
        if c > 0:
            run(give_side, c - 1)
        if c + 2 < chunks:
            send_chunk(c + 2)
        if c > 1:
            run(give_part, c - 2)
    last = of_chunk(chunks - 1)
    give_side(last[0])
    run(give_part, chunks - 2)
    for j in last[1:]:
        give_side(j)
    for j in last:
        give_part(j)
    for j in range(pieces):
        finish(j)

    first_all.wait_send()
    near_all.wait_send()
    slots_all.wait_send()
    for c in range(chunks):
        second_all(c).wait_send()
    for j in range(pieces):
        back_all(j).wait_send()
        side_copy(j).wait_send()
        part_copy(j).wait_send()
    for each in token_copies + route_copies:
        each.wait_send()


def keep_kernel(in_mats, out_mat, rows, gate_out, up_out, down_out, mixed, sem):
    chunks, _, block = out_mat.shape
    n_tp = block // 128
    lanes = block // n_tp
    down_cols = chunks * lanes
    copies = [
        (in_mats.at[0], gate_out.at[0]),
        (in_mats.at[1], up_out.at[0]),
        (rows, mixed),
    ]
    for c in range(chunks):
        for k in range(n_tp):
            start = k * down_cols + c * lanes
            copies.append(
                (
                    out_mat.at[c, :, k * lanes : (k + 1) * lanes],
                    down_out.at[0, :, start : start + lanes],
                )
            )
    copies = [
        pltpu.make_async_copy(source, target, sem.at[i])
        for i, (source, target) in enumerate(copies)
    ]
    for copy in copies:
        copy.start()
    for copy in copies:
        copy.wait()


def direct_shards(
    tokens, routes, route_weight, norm_gain, gate_weight, up_weight, down_weight
):
    n_fs, n_tp = lax.axis_size("fs"), lax.axis_size("tp")
    n = n_fs * n_tp
    tok_rows, width = tokens.shape
    tile_rows, tile_cols = gate_weight.shape[1:]
    down_rows, down_cols = down_weight.shape[1:]
    hidden = n_tp * tile_cols
    lanes = 128
    chunks = down_cols // lanes
    block = n_tp * lanes
    plane = n // 4
    splits = (2,) * chunks
    pieces = sum(splits)
    per_token = routes.shape[1]
    capacity = max(2, 3 * tok_rows * per_token // (2 * n))
    bf16, f32 = jnp.bfloat16, jnp.float32
    whole = pl.BlockSpec(memory_space=pltpu.VMEM)
    apart = pl.BlockSpec(memory_space=pltpu.HBM)
    dma = pltpu.SemaphoreType.DMA
    groups = 4
    in_mats, out_mat, rows = pl.pallas_call(
        functools.partial(exchange_kernel, (n_fs, n_tp, capacity, splits)),
        out_shape=(
            pltpu.VMEM((2, width, hidden), bf16),
            pltpu.VMEM((chunks, hidden, block), bf16),
            pltpu.VMEM((tok_rows, width), bf16),
        ),
        in_specs=[apart] * 7,
        out_specs=(whole, whole, whole),
        scratch_shapes=[
            pltpu.VMEM((tok_rows, width), tokens.dtype),
            pltpu.VMEM((per_token, tok_rows), routes.dtype),
            pltpu.VMEM((per_token, tok_rows), f32),
            pltpu.VMEM((tile_rows // lanes, lanes), f32),
            pltpu.VMEM((n, tile_rows, tile_cols), f32),
            pltpu.VMEM((n, tile_rows, tile_cols), f32),
            pltpu.VMEM((n, down_rows, down_cols), f32),
            pltpu.VMEM((tile_rows, tile_cols), f32),
            pltpu.VMEM((n, 2, tile_rows, tile_cols), bf16),
            pltpu.VMEM((n, chunks, down_rows, lanes), bf16),
            pltpu.VMEM((3, tok_rows, width), bf16),
            pltpu.VMEM((4, tok_rows, width), bf16),
            pltpu.VMEM((plane, 4, capacity, width), bf16),
            pltpu.VMEM((plane, 4, capacity, width), bf16),
            pltpu.VMEM((groups, n * capacity // groups, hidden), bf16),
            pltpu.VMEM((3, per_token, tok_rows), routes.dtype),
            pltpu.VMEM((3, per_token, tok_rows), f32),
            pltpu.VMEM((4, tok_rows, plane * capacity), bf16),
            pltpu.VMEM((4, tok_rows, plane * capacity), bf16),
            pltpu.VMEM((chunks, plane, 4, capacity, block), bf16),
            pltpu.VMEM((chunks, plane, 4, capacity, block), bf16),
            pltpu.VMEM((chunks, 2, tok_rows, block), bf16),
            pltpu.VMEM((chunks, 2, tok_rows, block), bf16),
            pltpu.VMEM((chunks, 2, tok_rows, block), f32),
            pltpu.VMEM((chunks, tok_rows, block), bf16),
            pltpu.VMEM((chunks, tok_rows, block), bf16),
            dma((7,)),
            dma((3,)),
            dma((3,)),
            dma((6,)),
            dma((6,)),
            dma,
            dma,
            dma,
            dma,
            dma,
            dma,
        ]
        + [dma((chunks,))] * 2
        + [dma((pieces,))] * 6
        + [pltpu.SemaphoreType.REGULAR((2,))],
        compiler_params=pltpu.CompilerParams(
            collective_id=0, has_side_effects=True, vmem_limit_bytes=52 * 1024 * 1024
        ),
    )(
        tokens,
        routes.T,
        route_weight.T,
        norm_gain.reshape(tile_rows // lanes, lanes),
        gate_weight,
        up_weight,
        down_weight,
    )
    return pl.pallas_call(
        keep_kernel,
        out_shape=(
            jax.ShapeDtypeStruct((1, width, hidden), bf16),
            jax.ShapeDtypeStruct((1, width, hidden), bf16),
            jax.ShapeDtypeStruct((1, hidden, width), bf16),
            jax.ShapeDtypeStruct((tok_rows, width), bf16),
        ),
        in_specs=[whole] * 3,
        out_specs=(apart,) * 4,
        scratch_shapes=[dma((3 + chunks * n_tp,))],
        compiler_params=pltpu.CompilerParams(vmem_limit_bytes=8 * 1024 * 1024),
    )(in_mats, out_mat, rows)


def aligned(mesh, tokens, routes, gate_weight, down_weight):
    n_fs, n_tp = mesh.shape["fs"], mesh.shape["tp"]
    n = n_fs * n_tp
    tok_rows = tokens.shape[0] // n
    capacity = max(2, 3 * tok_rows * routes.shape[1] // (2 * n))
    return (
        gate_weight.shape[0] == n
        and n_fs % 4 == 0
        and n % 32 == 0
        and capacity % 8 == 0
        and tok_rows % 128 == 0
        and tokens.shape[1] % 512 == 0
        and gate_weight.shape[1] // n_fs % 128 == 0
        and gate_weight.shape[2] // n_tp % 128 == 0
        and down_weight.shape[1] // n_fs % 16 == 0
        and down_weight.shape[2] // n_tp % 128 == 0
    )


def solution(mesh):
    placed = (
        P(("fs", "tp"), None),
        P(("fs", "tp"), None),
        P(("fs", "tp"), None),
        P("fs"),
        P(None, "fs", "tp"),
        P(None, "fs", "tp"),
        P(None, "fs", "tp"),
    )

    def run(tokens, routes, route_weight, norm_gain, gate_weight, up_weight, down_weight):
        direct = aligned(mesh, tokens, routes, gate_weight, down_weight)
        return jax.shard_map(
            direct_shards if direct else shards,
            mesh=mesh,
            in_specs=placed,
            out_specs=(
                P(("fs", "tp"), None, None),
                P(("fs", "tp"), None, None),
                P(("fs", "tp"), None, None),
                P(("fs", "tp"), None),
            ),
            check_vma=False,
        )(tokens, routes, route_weight, norm_gain, gate_weight, up_weight, down_weight)

    return run
```
